32 devices in a mesh: fs: 4 (over z), rep: 4 (over y, x), tp: 2 (over core).
Axes of the slice: x: 2, y: 2, z: 4, core: 2. Of those that a mesh axis runs over, the one named last changes fastest.
Arguments:
- normed_in: bfloat16 [24576, 2048], P(('fs', 'rep')), may hold values from -6 to 6
- cotan_rec: bfloat16 [24576, 2048], P(('fs', 'rep'), 'tp'), may hold values from -0.0390625 to 0.0390625
- cotan_gate: bfloat16 [24576, 2048], P(('fs', 'rep'), 'tp'), may hold values from -0.0390625 to 0.0390625
- factor_rec: bfloat16 [2048, 512], P('fs'), may hold values from -0.125 to 0.125
- factor_gate: bfloat16 [2048, 512], P('fs'), may hold values from -0.125 to 0.125
- first_rec: float32 [512, 2048], P('fs', 'tp'), may hold values from -6 to 6
- first_gate: float32 [512, 2048], P('fs', 'tp'), may hold values from -6 to 6
- second_rec: float32 [512, 2048], P('fs', 'tp'), may hold values from 0.25 to 4
- second_gate: float32 [512, 2048], P('fs', 'tp'), may hold values from 0.25 to 4
- master_rec: float32 [2048, 2048], P('fs', 'tp'), may hold values from -0.125 to 0.125
- master_gate: float32 [2048, 2048], P('fs', 'tp'), may hold values from -0.125 to 0.125
Outputs:
- update_rec: float32 [2048, 2048], P('fs', 'tp')
- update_gate: float32 [2048, 2048], P('fs', 'tp')
- new_first_rec: float32 [512, 2048], P('fs', 'tp')
- new_first_gate: float32 [512, 2048], P('fs', 'tp')
- new_second_rec: float32 [512, 2048], P('fs', 'tp')
- new_second_gate: float32 [512, 2048], P('fs', 'tp')
- copy_rec: bfloat16 [2048, 2048], P(None, 'tp')
- copy_gate: bfloat16 [2048, 2048], P(None, 'tp')
The draws below stay inside these ranges and needn't reach their ends.
All inputs are finite; a program needn't handle non-finite values.
Results may differ from the reference program's by a relative error of at most 0.007.
Values may be sent and summed in bfloat16 or wider, within the bound.
A program may use at most 128 MiB of HBM per device.

```python
import math
import jax
import jax.numpy as jnp
from jax import lax

D = 2048
DR = 2048
RANK = 512
TOKENS = 24576


def shard_levels(stream_key, shape, pieces, smallest, largest):
    loudness, own = 1.0, jax.random.fold_in(stream_key, 6)
    for axis_at, shards_of in pieces:
        heights = jnp.exp(jax.random.uniform(jax.random.fold_in(own, axis_at), (shards_of,), jnp.float32, smallest / len(pieces), largest / len(pieces)))
        loudness = loudness * jnp.repeat(heights, shape[axis_at] // shards_of).reshape([-1 if axis == axis_at else 1 for axis in range(len(shape))])
    return loudness


def centred(key, shape, scale, limit, cuts=(), dtype=jnp.bfloat16):
    factor_of = shard_levels(key, shape, cuts, -0.22, 0.18) if cuts else 1.0
    drawn = jax.random.normal(key, shape, jnp.float32) * scale * factor_of
    return jnp.minimum(jnp.maximum(drawn, -limit), limit).astype(dtype)


def setup_inputs(seed: int = 0) -> dict:
    key_of = jax.random.split(jax.random.key(seed), 12)
    return {
        "normed_in": centred(key_of[0], (TOKENS, D), 1.0, 6.0, ((0, 16),)),
        "cotan_rec": centred(key_of[1], (TOKENS, DR), (TOKENS ** -0.5), 0.0390625, ((0, 16), (1, 2))),
        "cotan_gate": centred(key_of[2], (TOKENS, DR), (TOKENS ** -0.5), 0.0390625, ((0, 16), (1, 2))),
        "factor_rec": centred(key_of[3], (D, RANK), D ** -0.5, 0.125, ((0, 4),)),
        "factor_gate": centred(key_of[4], (D, RANK), D ** -0.5, 0.125, ((0, 4),)),
        "first_rec": centred(key_of[5], (RANK, DR), 1.0, 6.0, ((0, 4), (1, 2)), jnp.float32),
        "first_gate": centred(key_of[6], (RANK, DR), 1.0, 6.0, ((0, 4), (1, 2)), jnp.float32),
        "second_rec": jnp.clip(jnp.exp(math.log(4.0) - 2.7725887 * jax.random.uniform(key_of[7], (RANK, DR), jnp.float32) ** shard_levels(key_of[7], (RANK, DR), ((0, 4), (1, 2)), -0.2, 0.2)), 0.25, 4.0),
        "second_gate": jnp.clip(jnp.exp(math.log(4.0) - 2.7725887 * jax.random.uniform(key_of[8], (RANK, DR), jnp.float32) ** shard_levels(key_of[8], (RANK, DR), ((0, 4), (1, 2)), -0.2, 0.2)), 0.25, 4.0),
        "master_rec": centred(key_of[9], (D, DR), D ** -0.5, 0.125, ((0, 4), (1, 2)), jnp.float32),
        "master_gate": centred(key_of[10], (D, DR), D ** -0.5, 0.125, ((0, 4), (1, 2)), jnp.float32),
    }


beta_first = 0.8
beta_second = 0.9
scale_floor = 0.25
step_rate = 0.01

def project_update(normed_in, cotan, factor, first, second, master):
    grad = lax.dot_general(normed_in, cotan, (((0,), (0,)), ((), ())), preferred_element_type=jnp.float32)
    factor_wide = factor.astype(jnp.float32)
    low = jnp.dot(factor_wide.T, grad, precision=lax.Precision.HIGHEST)
    new_first = beta_first * first + (1.0 - beta_first) * low
    new_second = beta_second * second + (1.0 - beta_second) * low * low
    direction = new_first / jnp.sqrt(new_second)
    scale = 1.0 / jnp.sqrt(jnp.mean(direction * direction) + scale_floor)
    update = jnp.dot(factor_wide, direction, precision=lax.Precision.HIGHEST) * scale
    copy = (master - step_rate * update).astype(jnp.bfloat16)
    return (update, new_first, new_second, copy)

def reference(normed_in, cotan_rec, cotan_gate, factor_rec, factor_gate, first_rec, first_gate, second_rec, second_gate, master_rec, master_gate):
    upd_rec, first_r, second_r, copy_rec = project_update(normed_in, cotan_rec, factor_rec, first_rec, second_rec, master_rec)
    upd_gate, first_g, second_g, copy_gate = project_update(normed_in, cotan_gate, factor_gate, first_gate, second_gate, master_gate)
    return (upd_rec, upd_gate, first_r, first_g, second_r, second_g, copy_rec, copy_gate)
```

```python
import functools

import jax
import jax.numpy as jnp
from jax import lax
from jax.experimental import pallas as pl
from jax.experimental.pallas import tpu as pltpu
from jax.sharding import PartitionSpec as P

beta_first = 0.8
beta_second = 0.9
scale_floor = 0.25
step_rate = 0.01

MESH = pl.DeviceIdType.MESH
F32 = jnp.float32
BF16 = jnp.bfloat16
TOKEN_TILES = 4
HALF_CHUNKS = 2
CHUNKS = 2 * HALF_CHUNKS
SHARES = {
    "factors": 0.0,
    "projection": 0.0,
    "products": 0.17,
    "stage": 0.34,
    "reduce": 0.42,
    "directions": 0.5,
    "gather": 1.0,
}


def kernel(
    nf,
    nr,
    x_hbm,
    c0_hbm,
    c1_hbm,
    fac0_hbm,
    fac1_hbm,
    first0,
    first1,
    second0,
    second1,
    mast0_hbm,
    mast1_hbm,
    fac_out,
    dir_out,
    low_out,
    mast_out,
    sum_out,
    x,
    c,
    fac,
    acc,
    proj,
    part,
    recv,
    keep,
    own,
    mid,
    recv_fs,
    fst,
    snd,
    low,
    dirs,
    wide,
    mast,
    sums,
    sums_z,
    sums_r,
    sums_t,
    local_sem,
    out_sem,
    oz_sem,
    op_sem,
    fz_s,
    fz_r,
    fp_s,
    fp_r,
    fd_s,
    fd_r,
    fx_s,
    fx_r,
    pj_s,
    pj_r,
    rp_s,
    rp_r,
    rf_s,
    rf_r,
    dz_s,
    dz_r,
    dp_s,
    dp_r,
    dd_s,
    dd_r,
    lw_s,
    lw_r,
    sz_s,
    sz_r,
    sr_s,
    sr_r,
    st_s,
    st_r,
    mz_s,
    mz_r,
    mp_s,
    mp_r,
):
    f, r, t = lax.axis_index("fs"), lax.axis_index("rep"), lax.axis_index("tp")
    tokens = x.shape[0]
    rank, cols = dirs.shape[1], dirs.shape[2]
    rows = fac0_hbm.shape[0]
    half, quarter = rows // 2, rows // nr
    low_rows = rank // nf
    low_half = low_rows // 2
    width = cols // nr
    tile = tokens // TOKEN_TILES
    side = nr // 2
    rx, ry = lax.rem(r, side), r // side
    across = (ry * side + 1 - rx, (1 - ry) * side + rx)
    corner = (1 - ry) * side + 1 - rx
    sibling = (f, r, 1 - t)

    def fpeer(k):
        return lax.rem(f + k, nf)

    def rpeer(k):
        return lax.rem(r + k, nr)

    def block(ff):
        return pl.ds(pl.multiple_of(ff * rows, rows), rows)

    mine = fac.at[t, block(f), :]

    @pl.when(t == 0)
    def _():
        pltpu.make_async_copy(fac0_hbm, mine, local_sem.at[0]).start()

    @pl.when(t != 0)
    def _():
        pltpu.make_async_copy(fac1_hbm, mine, local_sem.at[0]).start()

    load_m = [
        pltpu.make_async_copy(mast0_hbm, wide.at[0], local_sem.at[8]),
        pltpu.make_async_copy(mast1_hbm, wide.at[1], local_sem.at[9]),
    ]
    load_x = pltpu.make_async_copy(x_hbm, x, local_sem.at[1])
    for load in (*load_m, load_x):
        load.start()
    load_c = [
        pltpu.make_async_copy(c0_hbm, c.at[0], local_sem.at[2]),
        pltpu.make_async_copy(c1_hbm, c.at[1], local_sem.at[3]),
    ]
    lane = pl.ds(pl.multiple_of(r * width, width), width)
    load_s = []
    for i, (src, dst) in enumerate(
        ((first0, fst.at[0]), (first1, fst.at[1]), (second0, snd.at[0]), (second1, snd.at[1]))
    ):
        load_s.append(pltpu.make_async_copy(src.at[:, lane], dst, local_sem.at[4 + i]))
    for load in (*load_c, *load_s):
        load.start()

    barrier = pltpu.get_barrier_semaphore()
    for k in range(1, nf):
        pl.semaphore_signal(barrier, inc=1, device_id=(fpeer(k), r, t), device_id_type=MESH)
    for k in range(1, nr):
        pl.semaphore_signal(barrier, inc=1, device_id=(f, rpeer(k), t), device_id_type=MESH)
    pl.semaphore_signal(barrier, inc=1, device_id=sibling, device_id_type=MESH)
    pl.semaphore_wait(barrier, nf + nr - 1)

    started = []

    def remote(src, dst, s_sem, r_sem, device):
        return pltpu.make_async_remote_copy(
            src_ref=src, dst_ref=dst, send_sem=s_sem, recv_sem=r_sem,
            device_id=device, device_id_type=MESH,
        )

    def guarded(action, when):
        if when is None:
            action()
        else:
            pl.when(when)(lambda: action())

    def send(ref, s_sem, r_sem, device, dst=None, when=None):
        copy = remote(ref, ref if dst is None else dst, s_sem, r_sem, device)
        guarded(copy.start, when)
        started.append((copy, when))

    def arrived(ref, s_sem, r_sem, when=None):
        guarded(remote(ref, ref, s_sem, r_sem, sibling).wait_recv, when)

    outs = []

    def put(src, dst, sem, when=None):
        copy = pltpu.make_async_copy(src, dst, sem)
        guarded(copy.start, when)
        outs.append((copy, when))

    def fpiece(ff, rr, start=0, count=quarter):
        at = pl.multiple_of(ff * rows + rr * quarter + start, count)
        return fac.at[t, pl.ds(at, count), :]

    pltpu.make_async_copy(fac0_hbm, mine, local_sem.at[0]).wait()
    for k in range(1, nf):
        send(fpiece(f, r), fz_s.at[k - 1], fz_r.at[k - 1], (fpeer(k), r, t))

    chunk = half // HALF_CHUNKS
    line = (
        (lambda j: lax.rem(f + nf - j, nf), lambda j: f >= j, fpeer(1), f < nf - 1),
        (lambda j: lax.rem(f + j, nf), lambda j: f < nf - j, fpeer(nf - 1), f > 0),
    )

    def mpiece(ref, ff, ch, other=False):
        p = ch % 2
        h = rx if p == 0 else ry
        if other:
            h = 1 - h
        at = pl.multiple_of(ff * rows + h * half + (ch // 2) * chunk, chunk)
        return ref.at[p, pl.ds(at, chunk), :]

    for p in range(2):
        load_m[p].wait()
        mast[p, block(f), :] = wide[p].astype(BF16)
    for ch in range(CHUNKS):
        for d, (_, _, onto, there) in enumerate(line):
            send(mpiece(mast, f, ch), mz_s.at[d, 0, ch], mz_r.at[d, 0, ch], (onto, r, t), when=there)
    for p in range(2):
        put(mast.at[p, block(f), :], mast_out.at[p, block(f), :], out_sem.at[p])

    relays = [(j, ch) for j in range(1, nf) for ch in range(CHUNKS)]
    done = [0]

    def relay(point):
        upto = round(SHARES[point] * len(relays))
        for j, ch in relays[done[0]:upto]:
            for d, (source, exists, onto, there) in enumerate(line):
                piece = mpiece(mast, source(j), ch)
                arrived(piece, mz_s.at[d, j - 1, ch], mz_r.at[d, j - 1, ch], when=exists(j))
                if j < nf - 1:
                    send(piece, mz_s.at[d, j, ch], mz_r.at[d, j, ch], (onto, r, t), when=exists(j) & there)
                send(piece, mp_s.at[d, j - 1, ch], mp_r.at[d, j - 1, ch], (f, across[ch % 2], t), when=exists(j))
                put(piece, mpiece(mast_out, source(j), ch), oz_sem.at[d, j - 1, ch], when=exists(j))
        done[0] = max(done[0], upto)

    def project(ff, first=False):
        at = block(ff)
        for i in range(TOKEN_TILES):
            span = pl.ds(i * tile, tile)
            product = jnp.dot(x[span, at], fac[t, at, :], preferred_element_type=F32)
            acc[span, :] = product if first else acc[span, :] + product

    load_x.wait()
    project(f, first=True)

    for k in range(1, nf):
        src = fpeer(nf - k)
        arrived(fpiece(src, r), fz_s.at[k - 1], fz_r.at[k - 1])
        for a in range(2):
            send(fpiece(src, r), fp_s.at[a, k - 1], fp_r.at[a, k - 1], (f, across[a], t))
    fhalf = quarter // 2
    for k in range(1, nf):
        src = fpeer(nf - k)
        for a in range(2):
            arrived(fpiece(src, across[a]), fp_s.at[a, k - 1], fp_r.at[a, k - 1])
            send(
                fpiece(src, across[a], a * fhalf, fhalf), fd_s.at[a, k - 1], fd_r.at[a, k - 1],
                (f, across[1 - a], t),
            )
    relay("factors")
    for k in range(1, nf):
        src = fpeer(nf - k)
        for a in range(2):
            arrived(fpiece(src, corner, a * fhalf, fhalf), fd_s.at[a, k - 1], fd_r.at[a, k - 1])
        if k < nf - 1:
            project(src)
    at = block(fpeer(1))
    for i in range(TOKEN_TILES):
        span = pl.ds(i * tile, tile)
        product = jnp.dot(x[span, at], fac[t, at, :], preferred_element_type=F32)
        proj[t, :, span] = jnp.transpose(acc[span, :] + product).astype(BF16)
        send(proj.at[t, :, span], pj_s.at[i], pj_r.at[i], sibling)
    send(fac.at[t], fx_s, fx_r, sibling)
    relay("projection")
    for load in (*load_c, *load_s):
        load.wait()

    upper = rank // 2
    spans = (slice(0, upper), slice(upper, rank))

    def product(p, rr):
        at = pl.ds(pl.multiple_of(rr * width, width), width)
        return jnp.dot(proj[p], c[p, :, at], preferred_element_type=F32)

    def pass_part(s, m, a):
        send(part.at[s, m], rp_s.at[s, m], rp_r.at[s, m], (f, across[a], t), dst=recv.at[s, m])

    def got_part(s, m):
        arrived(recv.at[s, m], rp_s.at[s, m], rp_r.at[s, m])

    order = (t, 1 - t)
    for s, p in enumerate(order):
        if s == 1:
            for i in range(TOKEN_TILES):
                span = pl.ds(i * tile, tile)
                arrived(proj.at[1 - t, :, span], pj_s.at[i], pj_r.at[i])
        far = product(p, corner)
        for a in range(2):
            part[s, a] = far[spans[a]].astype(BF16)
            pass_part(s, a, a)
        for a in range(2):
            near = product(p, across[a])
            part[s, 2 + a] = near[spans[a]].astype(BF16)
            pass_part(s, 2 + a, a)
            keep[s, 1 - a] = near[spans[1 - a]]
        own[s] = product(p, r)
    relay("products")

    def rank_rows(ff):
        return pl.ds(pl.multiple_of(ff * low_rows, low_rows), low_rows)

    for s in range(2):
        for a in range(2):
            got_part(s, a)
            part[s, 4 + a] = (keep[s, a] + recv[s, a].astype(F32)).astype(BF16)
            pass_part(s, 4 + a, 1 - a)
    relay("stage")
    for s in range(2):
        for a in range(2):
            got_part(s, 2 + a)
            got_part(s, 4 + a)
            total = own[s, spans[a], :] + recv[s, 2 + a].astype(F32) + recv[s, 4 + a].astype(F32)
            own[s, spans[a], :] = total
            mid[s, spans[a], :] = total.astype(BF16)
        for k in range(1, nf):
            send(
                mid.at[s, rank_rows(fpeer(k)), :], rf_s.at[s, k - 1], rf_r.at[s, k - 1], (fpeer(k), r, t),
                dst=recv_fs.at[s, k - 1],
            )
    relay("reduce")

    def dpiece(p, ff, rr, start=0, count=low_rows):
        at = pl.ds(pl.multiple_of(rr * width, width), width)
        ranks = pl.ds(pl.multiple_of(ff * low_rows + start, count), count)
        return dirs.at[p, ranks, at]

    for s, p in enumerate(order):
        for k in range(1, nf):
            arrived(recv_fs.at[s, k - 1], rf_s.at[s, k - 1], rf_r.at[s, k - 1])
        total = own[s, rank_rows(f), :]
        for k in range(1, nf):
            total = total + recv_fs[s, k - 1].astype(F32)
        rounded = total.astype(BF16)
        low[p, :, lane] = rounded
        again = rounded.astype(F32)
        new_first = beta_first * fst[p] + (1.0 - beta_first) * again
        new_second = beta_second * snd[p] + (1.0 - beta_second) * again * again
        direction = (new_first / jnp.sqrt(new_second)).astype(BF16)
        dirs[p, rank_rows(f), lane] = direction
        for k in range(1, nf):
            send(dpiece(p, f, r), dz_s.at[s, k - 1], dz_r.at[s, k - 1], (fpeer(k), r, t))
        for a in range(2):
            send(dpiece(p, f, r), dp_s.at[s, a, 0], dp_r.at[s, a, 0], (f, across[a], t))
        square = direction.astype(F32)
        square = square * square
        square = jnp.sum(square.reshape(low_rows // 8, 8, width), axis=0)
        sums[p] = square
    for k in range(1, nf):
        send(sums, sz_s.at[k - 1], sz_r.at[k - 1], (fpeer(k), r, t), dst=sums_z.at[k - 1])
    relay("directions")
    for s, p in enumerate(order):
        for k in range(1, nf):
            src = fpeer(nf - k)
            arrived(dpiece(p, src, r), dz_s.at[s, k - 1], dz_r.at[s, k - 1])
            for a in range(2):
                send(dpiece(p, src, r), dp_s.at[s, a, k], dp_r.at[s, a, k], (f, across[a], t))
    for k in range(1, nf):
        arrived(sums_z.at[k - 1], sz_s.at[k - 1], sz_r.at[k - 1])
    total = sums[...]
    for k in range(1, nf):
        total = total + sums_z[k - 1]
    sums_r[0] = total
    for j in range(1, nr):
        send(sums_r.at[0], sr_s.at[j - 1], sr_r.at[j - 1], (f, rpeer(j), t), dst=sums_r.at[j])
    for s, p in enumerate(order):
        for k in range(nf):
            src = fpeer(nf - k) if k else f
            for a in range(2):
                arrived(dpiece(p, src, across[a]), dp_s.at[s, a, k], dp_r.at[s, a, k])
                send(
                    dpiece(p, src, across[a], a * low_half, low_half), dd_s.at[s, a, k], dd_r.at[s, a, k],
                    (f, across[1 - a], t),
                )
    for j in range(1, nr):
        send(low.at[:, :, lane], lw_s.at[j - 1], lw_r.at[j - 1], (f, rpeer(j), t))
    for j in range(1, nr):
        arrived(sums_r.at[j], sr_s.at[j - 1], sr_r.at[j - 1])
    total = sums_r[0]
    for j in range(1, nr):
        total = total + sums_r[j]
    sums_t[0] = total
    send(sums_t.at[0], st_s, st_r, sibling, dst=sums_t.at[1])
    arrived(fac.at[1 - t], fx_s, fx_r)
    put(fac, fac_out, out_sem.at[2])
    relay("gather")

    for s, p in enumerate(order):
        for k in range(nf):
            src = fpeer(nf - k) if k else f
            for a in range(2):
                arrived(dpiece(p, src, corner, a * low_half, low_half), dd_s.at[s, a, k], dd_r.at[s, a, k])
    put(dirs, dir_out, out_sem.at[3])
    arrived(sums_t.at[1], st_s, st_r)
    sum_out[...] = sums_t[0] + sums_t[1]
    for j in range(1, nr):
        rsrc = rpeer(nr - j)
        at = pl.ds(pl.multiple_of(rsrc * width, width), width)
        arrived(low.at[:, :, at], lw_s.at[j - 1], lw_r.at[j - 1])
    put(low, low_out, out_sem.at[4])
    for j, ch in relays:
        for d, (source, exists, _, _) in enumerate(line):
            piece = mpiece(mast, source(j), ch, other=True)
            arrived(piece, mp_s.at[d, j - 1, ch], mp_r.at[d, j - 1, ch], when=exists(j))
            put(piece, mpiece(mast_out, source(j), ch, other=True), op_sem.at[d, j - 1, ch], when=exists(j))
    for copy, when in outs:
        guarded(copy.wait, when)
    for copy, when in started:
        guarded(copy.wait_send, when)


def gather_all(nf, nr, normed_in, cotans, factors, firsts, seconds, masters):
    tokens, model = normed_in.shape
    cols = cotans[0].shape[1]
    rows, rank = factors[0].shape
    low_rows, width = rank // nf, cols // nr
    dma = pltpu.SemaphoreType.DMA
    anyspec = pl.BlockSpec(memory_space=pl.ANY)
    pair = lambda *shape: [dma(shape), dma(shape)]
    return pl.pallas_call(
        functools.partial(kernel, nf, nr),
        out_shape=(
            jax.ShapeDtypeStruct((2, model, rank), BF16),
            jax.ShapeDtypeStruct((2, rank, cols), BF16),
            jax.ShapeDtypeStruct((2, low_rows, cols), BF16),
            jax.ShapeDtypeStruct((2, model, cols), BF16),
            jax.ShapeDtypeStruct((2, 8, width), F32),
        ),
        in_specs=[anyspec] * 11,
        out_specs=(anyspec, anyspec, anyspec, anyspec, pl.BlockSpec(memory_space=pltpu.VMEM)),
        scratch_shapes=[
            pltpu.VMEM((tokens, model), BF16),
            pltpu.VMEM((2, tokens, cols), BF16),
            pltpu.VMEM((2, model, rank), BF16),
            pltpu.VMEM((tokens, rank), F32),
            pltpu.VMEM((2, rank, tokens), BF16),
            pltpu.VMEM((2, 6, rank // 2, width), BF16),
            pltpu.VMEM((2, 6, rank // 2, width), BF16),
            pltpu.VMEM((2, 2, rank // 2, width), F32),
            pltpu.VMEM((2, rank, width), F32),
            pltpu.VMEM((2, rank, width), BF16),
            pltpu.VMEM((2, nf - 1, low_rows, width), BF16),
            pltpu.VMEM((2, low_rows, width), F32),
            pltpu.VMEM((2, low_rows, width), F32),
            pltpu.VMEM((2, low_rows, cols), BF16),
            pltpu.VMEM((2, rank, cols), BF16),
            pltpu.VMEM((2, rows, cols), F32),
            pltpu.VMEM((2, model, cols), BF16),
            pltpu.VMEM((2, 8, width), F32),
            pltpu.VMEM((nf - 1, 2, 8, width), F32),
            pltpu.VMEM((nr, 2, 8, width), F32),
            pltpu.VMEM((2, 2, 8, width), F32),
            dma((10,)),
            dma((5,)),
            dma((2, nf - 1, CHUNKS)),
            dma((2, nf - 1, CHUNKS)),
            *pair(nf - 1),
            *pair(2, nf - 1),
            *pair(2, nf - 1),
            dma,
            dma,
            *pair(TOKEN_TILES),
            *pair(2, 6),
            *pair(2, nf - 1),
            *pair(2, nf - 1),
            *pair(2, 2, nf),
            *pair(2, 2, nf),
            *pair(nr - 1),
            *pair(nf - 1),
            *pair(nr - 1),
            dma,
            dma,
            *pair(2, nf - 1, CHUNKS),
            *pair(2, nf - 1, CHUNKS),
        ],
        cost_estimate=pl.CostEstimate(
            flops=10 * tokens * model * rank, bytes_accessed=400 * 2**20, transcendentals=0
        ),
        compiler_params=pltpu.CompilerParams(
            collective_id=0, has_side_effects=True, vmem_limit_bytes=60 * 2**20
        ),
    )(normed_in, *cotans, *factors, *firsts, *seconds, *masters)


def finish_kernel(
    nf,
    entries,
    where,
    scales,
    fac_hbm,
    dir_hbm,
    low_hbm,
    mast_hbm,
    first0,
    first1,
    second0,
    second1,
    upd0,
    upd1,
    nfirst0,
    nfirst1,
    nsecond0,
    nsecond1,
    copy0,
    copy1,
    fac,
    dirs,
    low,
    mast,
    upd,
    moments,
    fac_sem,
    mast_sem,
    dir_sem,
    mom_sem,
    copy_sem,
    upd_sem,
    mout_sem,
):
    f = where[0]
    model = mast.shape[1]
    rows = model // nf
    unit = min(rows, 256)
    per = rows // unit
    units = [(p, i, u) for p in range(2) for i in range(nf) for u in range(per)]

    def span(i, u):
        return pl.ds(pl.multiple_of(lax.rem(f + i, nf) * rows + u * unit, unit), unit)

    def load(n):
        p, i, u = units[n]
        return (
            pltpu.make_async_copy(fac_hbm.at[p, span(i, u), :], fac.at[p, span(i, u), :], fac_sem.at[n]),
            pltpu.make_async_copy(mast_hbm.at[p, span(i, u), :], mast.at[p, span(i, u), :], mast_sem.at[n]),
        )

    load_d = [pltpu.make_async_copy(dir_hbm.at[p], dirs.at[p], dir_sem.at[p]) for p in range(2)]
    loads = [load(n) for n in range(len(units))]
    load_m = [
        pltpu.make_async_copy(src, moments.at[i], mom_sem.at[i])
        for i, src in enumerate((first0, first1, second0, second1))
    ]
    load_l = pltpu.make_async_copy(low_hbm, low, mom_sem.at[4])
    load_d[0].start()
    for n, pair in enumerate(loads):
        for copy in pair:
            copy.start()
        if n == 1:
            load_d[1].start()
    for copy in (load_l, *load_m):
        copy.start()
    outs = []

    def put(src, dst, sem):
        copy = pltpu.make_async_copy(src, dst, sem)
        copy.start()
        outs.append(copy)

    for n, (p, i, u) in enumerate(units):
        if i == 0 and u == 0:
            load_d[p].wait()
        for copy in loads[n]:
            copy.wait()
        update = jnp.dot(fac[p, span(i, u), :], dirs[p], preferred_element_type=F32) * scales[p]
        if i == 0:
            upd[p, u * unit:(u + 1) * unit, :] = update
            put(
                upd.at[p, pl.ds(u * unit, unit), :], (upd0, upd1)[p].at[pl.ds(u * unit, unit), :],
                upd_sem.at[p, u],
            )
        mast[p, span(i, u), :] = (mast[p, span(i, u), :].astype(F32) - step_rate * update).astype(BF16)
        put(mast.at[p, span(i, u), :], (copy0, copy1)[p].at[span(i, u), :], copy_sem.at[n])
    load_l.wait()
    for copy in load_m:
        copy.wait()
    for p in range(2):
        again = low[p].astype(F32)
        moments[p] = beta_first * moments[p] + (1.0 - beta_first) * again
        put(moments.at[p], (nfirst0, nfirst1)[p], mout_sem.at[p])
        moments[2 + p] = beta_second * moments[2 + p] + (1.0 - beta_second) * again * again
        put(moments.at[2 + p], (nsecond0, nsecond1)[p], mout_sem.at[2 + p])
    for copy in outs:
        copy.wait()


def finish(nf, entries, where, scales, fac, dirs, low, mast, firsts, seconds):
    _, model, rank = fac.shape
    cols = dirs.shape[2]
    rows, low_rows = model // nf, low.shape[1]
    unit = min(rows, 256)
    count = 2 * (model // unit)
    dma = pltpu.SemaphoreType.DMA
    anyspec = pl.BlockSpec(memory_space=pl.ANY)
    smem = pl.BlockSpec(memory_space=pltpu.SMEM)
    shape = jax.ShapeDtypeStruct
    return pl.pallas_call(
        functools.partial(finish_kernel, nf, entries),
        out_shape=(
            *[shape((rows, cols), F32)] * 2,
            *[shape((low_rows, cols), F32)] * 4,
            *[shape((model, cols), BF16)] * 2,
        ),
        in_specs=[smem, smem] + [anyspec] * 8,
        out_specs=(anyspec,) * 8,
        scratch_shapes=[
            pltpu.VMEM((2, model, rank), BF16),
            pltpu.VMEM((2, rank, cols), BF16),
            pltpu.VMEM((2, low_rows, cols), BF16),
            pltpu.VMEM((2, model, cols), BF16),
            pltpu.VMEM((2, rows, cols), F32),
            pltpu.VMEM((4, low_rows, cols), F32),
            dma((count,)),
            dma((count,)),
            dma((2,)),
            dma((5,)),
            dma((count,)),
            dma((2, rows // unit)),
            dma((4,)),
        ],
        cost_estimate=pl.CostEstimate(
            flops=4 * model * rank * cols, bytes_accessed=30 * 2**20, transcendentals=0
        ),
        compiler_params=pltpu.CompilerParams(vmem_limit_bytes=60 * 2**20),
    )(where, scales, fac, dirs, low, mast, *firsts, *seconds)


def body(
    nf,
    nr,
    nt,
    normed_in,
    cotan_rec,
    cotan_gate,
    factor_rec,
    factor_gate,
    first_rec,
    first_gate,
    second_rec,
    second_gate,
    master_rec,
    master_gate,
):
    factors = (factor_rec, factor_gate)
    firsts = (first_rec, first_gate)
    seconds = (second_rec, second_gate)
    fac, dirs, low, mast, sums = gather_all(
        nf, nr, normed_in, (cotan_rec, cotan_gate), factors, firsts, seconds, (master_rec, master_gate)
    )
    entries = float(dirs.shape[1] * dirs.shape[2] * nt)
    scales = 1.0 / jnp.sqrt(jnp.sum(sums, axis=(1, 2)) / entries + scale_floor)
    where = lax.axis_index("fs").astype(jnp.int32).reshape(1)
    return finish(nf, entries, where, scales, fac, dirs, low, mast, firsts, seconds)


def solution(mesh):
    nf, nr, nt = mesh.shape["fs"], mesh.shape["rep"], mesh.shape["tp"]
    rows = P("fs", "tp")
    return jax.shard_map(
        functools.partial(body, nf, nr, nt),
        mesh=mesh,
        in_specs=(
            P(("fs", "rep"), None),
            P(("fs", "rep"), "tp"),
            P(("fs", "rep"), "tp"),
            P("fs", None),
            P("fs", None),
            *[rows] * 6,
        ),
        out_specs=(*[rows] * 6, P(None, "tp"), P(None, "tp")),
        check_vma=False,
    )
```

```python
import functools

import jax
import jax.numpy as jnp
from jax import lax
from jax.experimental import pallas as pl
from jax.experimental.pallas import tpu as pltpu
from jax.sharding import PartitionSpec as P

beta_first = 0.8
beta_second = 0.9
scale_floor = 0.25
step_rate = 0.01

MESH = pl.DeviceIdType.MESH
F32 = jnp.float32
BF16 = jnp.bfloat16
TOKEN_TILES = 4
HALF_CHUNKS = 2
CHUNKS = 2 * HALF_CHUNKS
SHARES = {
    "projection": (0.0, 0.17, 0.08, 0.0),
    "products": (0.0, 0.25, 0.08, 0.0),
    "stage": (0.0, 0.33, 0.08, 0.0),
    "reduce": (0.5, 0.42, 0.17, 0.33),
    "directions": (0.5, 0.42, 0.17, 0.33),
    "gather_z": (0.67, 0.5, 0.33, 0.33),
    "gather": (0.83, 0.67, 0.67, 0.67),
    "end": (1.0, 1.0, 1.0, 1.0),
}


def kernel(
    nf,
    nr,
    entries,
    x_hbm,
    c0_hbm,
    c1_hbm,
    fac0_hbm,
    fac1_hbm,
    first0,
    first1,
    second0,
    second1,
    mast0_hbm,
    mast1_hbm,
    fresh,
    upd,
    moments,
    x,
    c,
    fac,
    acc,
    proj,
    part,
    recv,
    keep,
    own,
    mid,
    recv_fs,
    low,
    dirs,
    mast,
    sums,
    sums_z,
    sums_r,
    sums_t,
    local_sem,
    fz_s,
    fz_r,
    fp_s,
    fp_r,
    fd_s,
    fd_r,
    fx_s,
    fx_r,
    pj_s,
    pj_r,
    rp_s,
    rp_r,
    rf_s,
    rf_r,
    dz_s,
    dz_r,
    dp_s,
    dp_r,
    dd_s,
    dd_r,
    lw_s,
    lw_r,
    sz_s,
    sz_r,
    sr_s,
    sr_r,
    st_s,
    st_r,
    mz_s,
    mz_r,
    mp_s,
    mp_r,
):
    f, r, t = lax.axis_index("fs"), lax.axis_index("rep"), lax.axis_index("tp")
    tokens = x.shape[0]
    rank, cols = dirs.shape[1], dirs.shape[2]
    rows = fac0_hbm.shape[0]
    half, quarter = rows // 2, rows // nr
    low_rows = rank // nf
    low_half = low_rows // 2
    width = cols // nr
    tile = tokens // TOKEN_TILES
    side = nr // 2
    rx, ry = lax.rem(r, side), r // side
    across = (ry * side + 1 - rx, (1 - ry) * side + rx)
    corner = (1 - ry) * side + 1 - rx
    sibling = (f, r, 1 - t)

    def fpeer(k):
        return lax.rem(f + k, nf)

    def rpeer(k):
        return lax.rem(r + k, nr)

    def block(ff):
        return pl.ds(pl.multiple_of(ff * rows, rows), rows)

    mine = fac.at[t, block(f), :]

    @pl.when(t == 0)
    def _():
        pltpu.make_async_copy(fac0_hbm, mine, local_sem.at[0]).start()

    @pl.when(t != 0)
    def _():
        pltpu.make_async_copy(fac1_hbm, mine, local_sem.at[0]).start()

    load_m = [
        pltpu.make_async_copy(mast0_hbm, upd.at[0], local_sem.at[8]),
        pltpu.make_async_copy(mast1_hbm, upd.at[1], local_sem.at[9]),
    ]
    load_x = pltpu.make_async_copy(x_hbm, x, local_sem.at[1])
    for load in (*load_m, load_x):
        load.start()
    load_c = [
        pltpu.make_async_copy(c0_hbm, c.at[0], local_sem.at[2]),
        pltpu.make_async_copy(c1_hbm, c.at[1], local_sem.at[3]),
    ]
    lane = pl.ds(pl.multiple_of(r * width, width), width)
    load_s = [
        pltpu.make_async_copy(src, moments.at[i], local_sem.at[4 + i])
        for i, src in enumerate((first0, first1, second0, second1))
    ]
    for load in (*load_c, *load_s):
        load.start()

    barrier = pltpu.get_barrier_semaphore()
    for k in range(1, nf):
        pl.semaphore_signal(barrier, inc=1, device_id=(fpeer(k), r, t), device_id_type=MESH)
    for k in range(1, nr):
        pl.semaphore_signal(barrier, inc=1, device_id=(f, rpeer(k), t), device_id_type=MESH)
    pl.semaphore_signal(barrier, inc=1, device_id=sibling, device_id_type=MESH)
    pl.semaphore_wait(barrier, nf + nr - 1)

    started = []

    def remote(src, dst, s_sem, r_sem, device):
        return pltpu.make_async_remote_copy(
            src_ref=src, dst_ref=dst, send_sem=s_sem, recv_sem=r_sem,
            device_id=device, device_id_type=MESH,
        )

    def guarded(action, when):
        if when is None:
            action()
        else:
            pl.when(when)(lambda: action())

    def send(ref, s_sem, r_sem, device, dst=None, when=None):
        copy = remote(ref, ref if dst is None else dst, s_sem, r_sem, device)
        guarded(copy.start, when)
        started.append((copy, when))

    def arrived(ref, s_sem, r_sem, when=None):
        guarded(remote(ref, ref, s_sem, r_sem, sibling).wait_recv, when)

    def fpiece(ff, rr, start=0, count=quarter):
        at = pl.multiple_of(ff * rows + rr * quarter + start, count)
        return fac.at[t, pl.ds(at, count), :]

    pltpu.make_async_copy(fac0_hbm, mine, local_sem.at[0]).wait()
    for k in range(1, nf):
        send(fpiece(f, r), fz_s.at[k - 1], fz_r.at[k - 1], (fpeer(k), r, t))

    chunk = half // HALF_CHUNKS
    line = (
        (lambda j: lax.rem(f + nf - j, nf), lambda j: f >= j, fpeer(1), f < nf - 1),
        (lambda j: lax.rem(f + j, nf), lambda j: f < nf - j, fpeer(nf - 1), f > 0),
    )

    def mrange(ff, ch, other=False):
        h = rx if ch % 2 == 0 else ry
        if other:
            h = 1 - h
        return ff * rows + h * half + (ch // 2) * chunk, chunk

    def mpiece(ff, ch, other=False):
        start, count = mrange(ff, ch, other)
        return mast.at[ch % 2, pl.ds(pl.multiple_of(start, count), count), :]

    def my_turn(ch):
        return (ry if ch % 2 == 0 else rx) == ch // 2

    def swap():
        for d, (source, exists, _, there) in enumerate(line):
            for ch in range(CHUNKS):
                piece = mpiece(source(1), ch)
                mine_first = exists(1) & jnp.logical_not(there) & my_turn(ch)
                arrived(piece, mz_s.at[d, 0, ch], mz_r.at[d, 0, ch], when=mine_first)
                send(
                    piece, mz_s.at[d, 1, ch], mz_r.at[d, 0, ch], (f, across[1 - ch % 2], t),
                    when=mine_first,
                )

    for p in range(2):
        load_m[p].wait()
        mast[p, block(f), :] = upd[p].astype(BF16)
    for ch in range(CHUNKS):
        for d, (_, _, onto, there) in enumerate(line):
            to_end = f == (nf - 2 if d == 0 else 1)
            send(
                mpiece(f, ch), mz_s.at[d, 0, ch], mz_r.at[d, 0, ch], (onto, r, t),
                when=there & (jnp.logical_not(to_end) | my_turn(ch)),
            )

    relays = [(j, ch) for j in range(1, nf) for ch in range(CHUNKS)]
    done = [0, 0, 0, 0]
    last = jnp.logical_or(f == 0, f == nf - 1)
    inner = jnp.logical_not(last)

    def land(j, ch, when, swapped=False):
        for d, (source, exists, _, there) in enumerate(line):
            due = exists(j) & when
            if j == 1:
                due = due & (jnp.logical_not(there | my_turn(ch)) if swapped else there)
            elif swapped:
                continue
            piece = mpiece(source(j), ch)
            arrived(piece, mz_s.at[d, j - 1, ch], mz_r.at[d, j - 1, ch], when=due)

    def onward(j, ch, ending):
        if j == nf - 1:
            return
        for d, (source, exists, onto, there) in enumerate(line):
            to_end = f == (nf - 2 if d == 0 else 1)
            if not ending:
                to_end = jnp.logical_not(to_end)
            send(
                mpiece(source(j), ch), mz_s.at[d, j, ch], mz_r.at[d, j, ch], (onto, r, t),
                when=exists(j) & there & inner & to_end,
            )

    def aside(j, ch, when):
        for d, (source, exists, _, _) in enumerate(line):
            piece = mpiece(source(j), ch)
            send(
                piece, mp_s.at[d, j - 1, ch], mp_r.at[d, j - 1, ch], (f, across[ch % 2], t),
                when=exists(j) & when,
            )

    def relay(point):
        ends = [max(d, round(share * len(relays))) for d, share in zip(done, SHARES[point])]
        for n in range(done[0], ends[0]):
            land(*relays[n], last)
            land(*relays[n], last, swapped=True)
            aside(*relays[n], last)
        landed = max(done[1:])
        for n in range(min(done[1:]), max(ends[1:])):
            if n >= landed:
                land(*relays[n], inner)
            if done[1] <= n < ends[1]:
                onward(*relays[n], True)
            if done[2] <= n < ends[2]:
                onward(*relays[n], False)
            if done[3] <= n < ends[3]:
                aside(*relays[n], inner)
        done[:] = ends

    def project(ff, first=False):
        at = block(ff)
        for i in range(TOKEN_TILES):
            span = pl.ds(i * tile, tile)
            product = jnp.dot(x[span, at], fac[t, at, :], preferred_element_type=F32)
            acc[span, :] = product if first else acc[span, :] + product

    load_x.wait()
    project(f, first=True)

    for k in range(1, nf):
        src = fpeer(nf - k)
        arrived(fpiece(src, r), fz_s.at[k - 1], fz_r.at[k - 1])
        for a in range(2):
            send(fpiece(src, r), fp_s.at[a, k - 1], fp_r.at[a, k - 1], (f, across[a], t))
    fhalf = quarter // 2
    for k in range(1, nf):
        src = fpeer(nf - k)
        for a in range(2):
            arrived(fpiece(src, across[a]), fp_s.at[a, k - 1], fp_r.at[a, k - 1])
            send(
                fpiece(src, across[a], a * fhalf, fhalf), fd_s.at[a, k - 1], fd_r.at[a, k - 1],
                (f, across[1 - a], t),
            )
    def corner_arrived(k):
        for a in range(2):
            piece = fpiece(fpeer(nf - k), corner, a * fhalf, fhalf)
            arrived(piece, fd_s.at[a, k - 1], fd_r.at[a, k - 1])

    @pl.loop(1, nf - 1)
    def _(k):
        corner_arrived(k)
        project(fpeer(nf - k))

    corner_arrived(nf - 1)
    at = block(fpeer(1))
    for i in range(TOKEN_TILES):
        span = pl.ds(i * tile, tile)
        product = jnp.dot(x[span, at], fac[t, at, :], preferred_element_type=F32)
        proj[t, :, span] = jnp.transpose(acc[span, :] + product).astype(BF16)
        send(proj.at[t, :, span], pj_s.at[i], pj_r.at[i], sibling)
    send(fac.at[t], fx_s, fx_r, sibling)
    relay("projection")
    for load in (*load_c, *load_s):
        load.wait()

    upper = rank // 2
    spans = (slice(0, upper), slice(upper, rank))

    def product(p, rr):
        at = pl.ds(pl.multiple_of(rr * width, width), width)
        return jnp.dot(proj[p], c[p, :, at], preferred_element_type=F32)

    def pass_part(s, m, a):
        send(part.at[s, m], rp_s.at[s, m], rp_r.at[s, m], (f, across[a], t), dst=recv.at[s, m])

    def got_part(s, m):
        arrived(recv.at[s, m], rp_s.at[s, m], rp_r.at[s, m])

    order = (t, 1 - t)
    for s, p in enumerate(order):
        if s == 1:
            for i in range(TOKEN_TILES):
                span = pl.ds(i * tile, tile)
                arrived(proj.at[1 - t, :, span], pj_s.at[i], pj_r.at[i])
        far = product(p, corner)
        for a in range(2):
            part[s, a] = far[spans[a]].astype(BF16)
            pass_part(s, a, a)
        for a in range(2):
            near = product(p, across[a])
            part[s, 2 + a] = near[spans[a]].astype(BF16)
            pass_part(s, 2 + a, a)
            keep[s, 1 - a] = near[spans[1 - a]]
        own[s] = product(p, r)
    relay("products")

    def rank_rows(ff):
        return pl.ds(pl.multiple_of(ff * low_rows, low_rows), low_rows)

    for s in range(2):
        for a in range(2):
            got_part(s, a)
            part[s, 4 + a] = (keep[s, a] + recv[s, a].astype(F32)).astype(BF16)
            pass_part(s, 4 + a, 1 - a)
    swap()
    relay("stage")
    for s in range(2):
        for a in range(2):
            got_part(s, 2 + a)
            got_part(s, 4 + a)
            total = own[s, spans[a], :] + recv[s, 2 + a].astype(F32) + recv[s, 4 + a].astype(F32)
            own[s, spans[a], :] = total
            mid[s, spans[a], :] = total.astype(BF16)
        for k in range(1, nf):
            send(
                mid.at[s, rank_rows(fpeer(k)), :], rf_s.at[s, k - 1], rf_r.at[s, k - 1], (fpeer(k), r, t),
                dst=recv_fs.at[s, k - 1],
            )
    relay("reduce")

    def dpiece(p, ff, rr, start=0, count=low_rows):
        at = pl.ds(pl.multiple_of(rr * width, width), width)
        ranks = pl.ds(pl.multiple_of(ff * low_rows + start, count), count)
        return dirs.at[p, ranks, at]

    for s, p in enumerate(order):
        for k in range(1, nf):
            arrived(recv_fs.at[s, k - 1], rf_s.at[s, k - 1], rf_r.at[s, k - 1])
        total = own[s, rank_rows(f), :]
        for k in range(1, nf):
            total = total + recv_fs[s, k - 1].astype(F32)
        rounded = total.astype(BF16)
        low[p, :, lane] = rounded
        again = rounded.astype(F32)
        new_first = beta_first * moments[p, :, lane] + (1.0 - beta_first) * again
        new_second = beta_second * moments[2 + p, :, lane] + (1.0 - beta_second) * again * again
        direction = (new_first / jnp.sqrt(new_second)).astype(BF16)
        dirs[p, rank_rows(f), lane] = direction
        for k in range(1, nf):
            send(dpiece(p, f, r), dz_s.at[s, k - 1], dz_r.at[s, k - 1], (fpeer(k), r, t))
        for a in range(2):
            send(dpiece(p, f, r), dp_s.at[s, a, 0], dp_r.at[s, a, 0], (f, across[a], t))
        square = direction.astype(F32)
        square = square * square
        square = jnp.sum(square.reshape(low_rows // 8, 8, width), axis=0)
        sums[p] = square
    for k in range(1, nf):
        send(sums, sz_s.at[k - 1], sz_r.at[k - 1], (fpeer(k), r, t), dst=sums_z.at[k - 1])
    relay("directions")
    for s, p in enumerate(order):
        for k in range(1, nf):
            src = fpeer(nf - k)
            arrived(dpiece(p, src, r), dz_s.at[s, k - 1], dz_r.at[s, k - 1])
            for a in range(2):
                send(dpiece(p, src, r), dp_s.at[s, a, k], dp_r.at[s, a, k], (f, across[a], t))
    relay("gather_z")
    for k in range(1, nf):
        arrived(sums_z.at[k - 1], sz_s.at[k - 1], sz_r.at[k - 1])
    total = sums[...]
    for k in range(1, nf):
        total = total + sums_z[k - 1]
    sums_r[0] = total
    for j in range(1, nr):
        send(sums_r.at[0], sr_s.at[j - 1], sr_r.at[j - 1], (f, rpeer(j), t), dst=sums_r.at[j])
    for s, p in enumerate(order):
        for k in range(nf):
            src = fpeer(nf - k) if k else f
            for a in range(2):
                arrived(dpiece(p, src, across[a]), dp_s.at[s, a, k], dp_r.at[s, a, k])
                send(
                    dpiece(p, src, across[a], a * low_half, low_half), dd_s.at[s, a, k], dd_r.at[s, a, k],
                    (f, across[1 - a], t),
                )
    for j in range(1, nr):
        send(low.at[:, :, lane], lw_s.at[j - 1], lw_r.at[j - 1], (f, rpeer(j), t))
    for j in range(1, nr):
        arrived(sums_r.at[j], sr_s.at[j - 1], sr_r.at[j - 1])
    total = sums_r[0]
    for j in range(1, nr):
        total = total + sums_r[j]
    sums_t[0] = total
    send(sums_t.at[0], st_s, st_r, sibling, dst=sums_t.at[1])
    arrived(fac.at[1 - t], fx_s, fx_r)
    relay("gather")

    for s, p in enumerate(order):
        for k in range(nf):
            src = fpeer(nf - k) if k else f
            for a in range(2):
                arrived(dpiece(p, src, corner, a * low_half, low_half), dd_s.at[s, a, k], dd_r.at[s, a, k])
    relay("end")
    arrived(sums_t.at[1], st_s, st_r)
    total = sums_t[0] + sums_t[1]
    scales = [1.0 / jnp.sqrt(jnp.sum(total[p]) / entries + scale_floor) for p in range(2)]

    def update_of(p, at):
        return jnp.dot(fac[p, at, :], dirs[p], preferred_element_type=F32) * scales[p]

    def renew(p, start, count):
        at = pl.ds(pl.multiple_of(start, count), count)
        fresh[p, at, :] = (mast[p, at, :].astype(F32) - step_rate * update_of(p, at)).astype(BF16)

    unit = min(rows, 256)

    def renew_block(ff):
        for p in range(2):
            for i in range(rows // unit):
                renew(p, ff * rows + i * unit, unit)

    for p in range(2):
        for i in range(rows // unit):
            at = pl.ds(pl.multiple_of(f * rows + i * unit, unit), unit)
            update = update_of(p, at)
            span = pl.ds(i * unit, unit)
            fresh[p, at, :] = (mast[p, at, :].astype(F32) - step_rate * update).astype(BF16)
            upd[p, span, :] = update
    for j in range(1, nr):
        rsrc = rpeer(nr - j)
        at = pl.ds(pl.multiple_of(rsrc * width, width), width)
        arrived(low.at[:, :, at], lw_s.at[j - 1], lw_r.at[j - 1])
    for p in range(2):
        again = low[p].astype(F32)
        moments[p] = beta_first * moments[p] + (1.0 - beta_first) * again
        moments[2 + p] = beta_second * moments[2 + p] + (1.0 - beta_second) * again * again

    def beside(j, ch, d):
        source, exists, _, _ = line[d]
        piece = mpiece(source(j), ch, other=True)
        arrived(piece, mp_s.at[d, j - 1, ch], mp_r.at[d, j - 1, ch], when=exists(j))

    @pl.loop(1, nf - 1)
    def _(j):
        for d, (source, exists, _, _) in enumerate(line):
            for ch in range(CHUNKS):
                beside(j, ch, d)
            guarded(lambda: renew_block(source(j)), exists(j))

    j = nf - 1
    for ch in range(CHUNKS):
        for d, (source, exists, _, _) in enumerate(line):
            start, count = mrange(source(j), ch)
            guarded(lambda: renew(ch % 2, start, count), exists(j))
    for ch in range(CHUNKS):
        for d, (source, exists, _, _) in enumerate(line):
            beside(j, ch, d)
            start, count = mrange(source(j), ch, other=True)
            guarded(lambda: renew(ch % 2, start, count), exists(j))
    for copy, when in started:
        guarded(copy.wait_send, when)


def gather_all(nf, nr, entries, normed_in, cotans, factors, firsts, seconds, masters):
    tokens, model = normed_in.shape
    cols = cotans[0].shape[1]
    rows, rank = factors[0].shape
    low_rows, width = rank // nf, cols // nr
    dma = pltpu.SemaphoreType.DMA
    anyspec = pl.BlockSpec(memory_space=pl.ANY)
    pair = lambda *shape: [dma(shape), dma(shape)]
    return pl.pallas_call(
        functools.partial(kernel, nf, nr, entries),
        out_shape=(
            pltpu.VMEM((2, model, cols), BF16),
            pltpu.VMEM((2, rows, cols), F32),
            pltpu.VMEM((4, low_rows, cols), F32),
        ),
        in_specs=[anyspec] * 11,
        out_specs=(pl.BlockSpec(memory_space=pltpu.VMEM),) * 3,
        scratch_shapes=[
            pltpu.VMEM((tokens, model), BF16),
            pltpu.VMEM((2, tokens, cols), BF16),
            pltpu.VMEM((2, model, rank), BF16),
            pltpu.VMEM((tokens, rank), F32),
            pltpu.VMEM((2, rank, tokens), BF16),
            pltpu.VMEM((2, 6, rank // 2, width), BF16),
            pltpu.VMEM((2, 6, rank // 2, width), BF16),
            pltpu.VMEM((2, 2, rank // 2, width), F32),
            pltpu.VMEM((2, rank, width), F32),
            pltpu.VMEM((2, rank, width), BF16),
            pltpu.VMEM((2, nf - 1, low_rows, width), BF16),
            pltpu.VMEM((2, low_rows, cols), BF16),
            pltpu.VMEM((2, rank, cols), BF16),
            pltpu.VMEM((2, model, cols), BF16),
            pltpu.VMEM((2, 8, width), F32),
            pltpu.VMEM((nf - 1, 2, 8, width), F32),
            pltpu.VMEM((nr, 2, 8, width), F32),
            pltpu.VMEM((2, 2, 8, width), F32),
            dma((10,)),
            *pair(nf - 1),
            *pair(2, nf - 1),
            *pair(2, nf - 1),
            dma,
            dma,
            *pair(TOKEN_TILES),
            *pair(2, 6),
            *pair(2, nf - 1),
            *pair(2, nf - 1),
            *pair(2, 2, nf),
            *pair(2, 2, nf),
            *pair(nr - 1),
            *pair(nf - 1),
            *pair(nr - 1),
            dma,
            dma,
            *pair(2, nf - 1, CHUNKS),
            *pair(2, nf - 1, CHUNKS),
        ],
        cost_estimate=pl.CostEstimate(
            flops=10 * tokens * model * rank, bytes_accessed=400 * 2**20, transcendentals=0
        ),
        compiler_params=pltpu.CompilerParams(
            collective_id=0, has_side_effects=True, vmem_limit_bytes=46 * 2**20
        ),
    )(normed_in, *cotans, *factors, *firsts, *seconds, *masters)


def finish_kernel(fresh, upd, moments, *rest):
    outs, sem = rest[:-1], rest[-1]
    pieces = [(upd.at[p], outs[p]) for p in range(2)]
    pieces += [(moments.at[i], outs[2 + i]) for i in range(4)]
    share = fresh.shape[1] // 4
    for p in range(2):
        for i in range(4):
            span = pl.ds(i * share, share)
            pieces.append((fresh.at[p, span, :], outs[6 + p].at[span, :]))
    copies = [pltpu.make_async_copy(src, dst, sem.at[i]) for i, (src, dst) in enumerate(pieces)]
    for copy in copies:
        copy.start()
    for copy in copies:
        copy.wait()


def finish(fresh, upd, moments):
    shape = jax.ShapeDtypeStruct
    anyspec = pl.BlockSpec(memory_space=pl.ANY)
    return pl.pallas_call(
        finish_kernel,
        out_shape=(
            *[shape(upd.shape[1:], F32)] * 2,
            *[shape(moments.shape[1:], F32)] * 4,
            *[shape(fresh.shape[1:], BF16)] * 2,
        ),
        in_specs=[pl.BlockSpec(memory_space=pltpu.VMEM)] * 3,
        out_specs=(anyspec,) * 8,
        scratch_shapes=[pltpu.SemaphoreType.DMA((14,))],
        cost_estimate=pl.CostEstimate(flops=0, bytes_accessed=14 * 2**20, transcendentals=0),
        compiler_params=pltpu.CompilerParams(vmem_limit_bytes=2**20),
    )(fresh, upd, moments)


def body(
    nf,
    nr,
    nt,
    normed_in,
    cotan_rec,
    cotan_gate,
    factor_rec,
    factor_gate,
    first_rec,
    first_gate,
    second_rec,
    second_gate,
    master_rec,
    master_gate,
):
    factors = (factor_rec, factor_gate)
    firsts = (first_rec, first_gate)
    seconds = (second_rec, second_gate)
    entries = float(factor_rec.shape[1] * cotan_rec.shape[1] * nt)
    return finish(
        *gather_all(
            nf, nr, entries, normed_in, (cotan_rec, cotan_gate), factors, firsts, seconds,
            (master_rec, master_gate),
        )
    )


def solution(mesh):
    nf, nr, nt = mesh.shape["fs"], mesh.shape["rep"], mesh.shape["tp"]
    rows = P("fs", "tp")
    return jax.shard_map(
        functools.partial(body, nf, nr, nt),
        mesh=mesh,
        in_specs=(
            P(("fs", "rep"), None),
            P(("fs", "rep"), "tp"),
            P(("fs", "rep"), "tp"),
            P("fs", None),
            P("fs", None),
            *[rows] * 6,
        ),
        out_specs=(*[rows] * 6, P(None, "tp"), P(None, "tp")),
        check_vma=False,
    )
```

```python
import functools

import jax
import jax.numpy as jnp
from jax import lax
from jax.experimental import pallas as pl
from jax.experimental.pallas import tpu as pltpu
from jax.sharding import PartitionSpec as P

beta_first = 0.8
beta_second = 0.9
scale_floor = 0.25
step_rate = 0.01

MESH = pl.DeviceIdType.MESH
F32 = jnp.float32
BF16 = jnp.bfloat16
TOKEN_TILES = 4
HALF_CHUNKS = 2
CHUNKS = 2 * HALF_CHUNKS
SHARES = {
    "projection": (0.0, 0.17, 0.08, 0.0),
    "products": (0.0, 0.25, 0.08, 0.0),
    "stage": (0.0, 0.33, 0.08, 0.0),
    "reduce": (0.5, 0.42, 0.17, 0.33),
    "directions": (0.5, 0.42, 0.17, 0.33),
    "gather_z": (0.58, 0.5, 0.33, 0.33),
    "gather": (0.83, 0.67, 0.67, 0.67),
    "end": (1.0, 1.0, 1.0, 1.0),
}


def kernel(
    nf,
    nr,
    entries,
    x_hbm,
    c0_hbm,
    c1_hbm,
    fac0_hbm,
    fac1_hbm,
    first0,
    first1,
    second0,
    second1,
    mast0_hbm,
    mast1_hbm,
    fresh,
    upd,
    moments,
    x,
    c,
    fac,
    acc,
    proj,
    part,
    recv,
    keep,
    own,
    mid,
    recv_fs,
    recv_end,
    joint,
    low,
    dirs,
    mast,
    sums,
    sums_z,
    sums_r,
    sums_t,
    local_sem,
    fz_s,
    fz_r,
    fp_s,
    fp_r,
    fd_s,
    fd_r,
    fx_s,
    fx_r,
    pj_s,
    pj_r,
    rp_s,
    rp_r,
    rf_s,
    rf_r,
    re_s,
    re_r,
    dz_s,
    dz_r,
    dp_s,
    dp_r,
    dd_s,
    dd_r,
    lw_s,
    lw_r,
    sz_s,
    sz_r,
    sr_s,
    sr_r,
    st_s,
    st_r,
    mz_s,
    mz_r,
    mp_s,
    mp_r,
):
    f, r, t = lax.axis_index("fs"), lax.axis_index("rep"), lax.axis_index("tp")
    tokens = x.shape[0]
    rank, cols = dirs.shape[1], dirs.shape[2]
    rows = fac0_hbm.shape[0]
    half, quarter = rows // 2, rows // nr
    low_rows = rank // nf
    low_half = low_rows // 2
    width = cols // nr
    tile = tokens // TOKEN_TILES
    side = nr // 2
    rx, ry = lax.rem(r, side), r // side
    across = (ry * side + 1 - rx, (1 - ry) * side + rx)
    corner = (1 - ry) * side + 1 - rx
    sibling = (f, r, 1 - t)

    def fpeer(k):
        return lax.rem(f + k, nf)

    def rpeer(k):
        return lax.rem(r + k, nr)

    def block(ff):
        return pl.ds(pl.multiple_of(ff * rows, rows), rows)

    mine = fac.at[t, block(f), :]

    @pl.when(t == 0)
    def _():
        pltpu.make_async_copy(fac0_hbm, mine, local_sem.at[0]).start()

    @pl.when(t != 0)
    def _():
        pltpu.make_async_copy(fac1_hbm, mine, local_sem.at[0]).start()

    load_m = [
        pltpu.make_async_copy(mast0_hbm, upd.at[0], local_sem.at[8]),
        pltpu.make_async_copy(mast1_hbm, upd.at[1], local_sem.at[9]),
    ]
    load_x = pltpu.make_async_copy(x_hbm, x, local_sem.at[1])
    for load in (*load_m, load_x):
        load.start()
    load_c = [
        pltpu.make_async_copy(c0_hbm, c.at[0], local_sem.at[2]),
        pltpu.make_async_copy(c1_hbm, c.at[1], local_sem.at[3]),
    ]
    lane = pl.ds(pl.multiple_of(r * width, width), width)
    load_s = [
        pltpu.make_async_copy(src, moments.at[i], local_sem.at[4 + i])
        for i, src in enumerate((first0, first1, second0, second1))
    ]
    for load in (*load_c, *load_s):
        load.start()

    barrier = pltpu.get_barrier_semaphore()
    for k in range(1, nf):
        pl.semaphore_signal(barrier, inc=1, device_id=(fpeer(k), r, t), device_id_type=MESH)
    for k in range(1, nr):
        pl.semaphore_signal(barrier, inc=1, device_id=(f, rpeer(k), t), device_id_type=MESH)
    pl.semaphore_signal(barrier, inc=1, device_id=sibling, device_id_type=MESH)
    pl.semaphore_wait(barrier, nf + nr - 1)

    started = []

    def remote(src, dst, s_sem, r_sem, device):
        return pltpu.make_async_remote_copy(
            src_ref=src, dst_ref=dst, send_sem=s_sem, recv_sem=r_sem,
            device_id=device, device_id_type=MESH,
        )

    def guarded(action, when):
        if when is None:
            action()
        else:
            pl.when(when)(lambda: action())

    def send(ref, s_sem, r_sem, device, dst=None, when=None):
        copy = remote(ref, ref if dst is None else dst, s_sem, r_sem, device)
        guarded(copy.start, when)
        started.append((copy, when))

    def arrived(ref, s_sem, r_sem, when=None):
        guarded(remote(ref, ref, s_sem, r_sem, sibling).wait_recv, when)

    def fpiece(ff, rr, start=0, count=quarter):
        at = pl.multiple_of(ff * rows + rr * quarter + start, count)
        return fac.at[t, pl.ds(at, count), :]

    pltpu.make_async_copy(fac0_hbm, mine, local_sem.at[0]).wait()
    for k in range(1, nf):
        send(fpiece(f, r), fz_s.at[k - 1], fz_r.at[k - 1], (fpeer(k), r, t))

    chunk = half // HALF_CHUNKS
    line = (
        (lambda j: lax.rem(f + nf - j, nf), lambda j: f >= j, fpeer(1), f < nf - 1),
        (lambda j: lax.rem(f + j, nf), lambda j: f < nf - j, fpeer(nf - 1), f > 0),
    )

    def mrange(ff, ch, other=False):
        h = rx if ch % 2 == 0 else ry
        if other:
            h = 1 - h
        return ff * rows + h * half + (ch // 2) * chunk, chunk

    def mpiece(ff, ch, other=False):
        start, count = mrange(ff, ch, other)
        return mast.at[ch % 2, pl.ds(pl.multiple_of(start, count), count), :]

    def own_chunks(late, chunks=range(CHUNKS)):
        for ch in chunks:
            for d, (_, _, onto, there) in enumerate(line):
                to_end = f == (nf - 2 if d == 0 else 1)
                when = there
                if late:
                    when = there & to_end
                elif ch >= CHUNKS // 2:
                    when = there & jnp.logical_not(to_end)
                if ch >= CHUNKS // 2 or not late:
                    send(mpiece(f, ch), mz_s.at[d, 0, ch], mz_r.at[d, 0, ch], (onto, r, t), when=when)

    for p in range(2):
        load_m[p].wait()
        mast[p, block(f), :] = upd[p].astype(BF16)
    own_chunks(late=False)

    relays = [(j, ch) for j in range(1, nf) for ch in range(CHUNKS)]
    late = [(1, ch) for ch in range(CHUNKS // 2, CHUNKS)]
    final = relays[-(CHUNKS // 2):]
    relays_last = [n for n in relays if n not in late and n not in final]
    relays_last.insert(len(relays_last) - CHUNKS // 2, late[0])
    relays_last += late[1:] + final
    done = [0, 0, 0, 0]
    last = jnp.logical_or(f == 0, f == nf - 1)
    inner = jnp.logical_not(last)

    def land(j, ch, when):
        for d, (source, exists, _, _) in enumerate(line):
            piece = mpiece(source(j), ch)
            arrived(piece, mz_s.at[d, j - 1, ch], mz_r.at[d, j - 1, ch], when=exists(j) & when)

    def onward(j, ch, ending):
        if j == nf - 1:
            return
        for d, (source, exists, onto, there) in enumerate(line):
            to_end = f == (nf - 2 if d == 0 else 1)
            if not ending:
                to_end = jnp.logical_not(to_end)
            send(
                mpiece(source(j), ch), mz_s.at[d, j, ch], mz_r.at[d, j, ch], (onto, r, t),
                when=exists(j) & there & inner & to_end,
            )

    def aside(j, ch, when):
        for d, (source, exists, _, _) in enumerate(line):
            piece = mpiece(source(j), ch)
            send(
                piece, mp_s.at[d, j - 1, ch], mp_r.at[d, j - 1, ch], (f, across[ch % 2], t),
                when=exists(j) & when,
            )

    def relay(point):
        ends = [max(d, round(share * len(relays))) for d, share in zip(done, SHARES[point])]
        for n in range(done[0], ends[0]):
            land(*relays_last[n], last)
            aside(*relays_last[n], last)
        landed = max(done[1:])
        for n in range(min(done[1:]), max(ends[1:])):
            if n >= landed:
                land(*relays[n], inner)
            if done[1] <= n < ends[1]:
                onward(*relays[n], True)
            if done[2] <= n < ends[2]:
                onward(*relays[n], False)
            if done[3] <= n < ends[3]:
                aside(*relays[n], inner)
        done[:] = ends

    def project(ff, first=False):
        at = block(ff)
        for i in range(TOKEN_TILES):
            span = pl.ds(i * tile, tile)
            product = jnp.dot(x[span, at], fac[t, at, :], preferred_element_type=F32)
            acc[span, :] = product if first else acc[span, :] + product

    load_x.wait()
    project(f, first=True)

    for k in range(1, nf):
        src = fpeer(nf - k)
        arrived(fpiece(src, r), fz_s.at[k - 1], fz_r.at[k - 1])
        for a in range(2):
            send(fpiece(src, r), fp_s.at[a, k - 1], fp_r.at[a, k - 1], (f, across[a], t))
    fhalf = quarter // 2
    for k in range(1, nf):
        src = fpeer(nf - k)
        for a in range(2):
            arrived(fpiece(src, across[a]), fp_s.at[a, k - 1], fp_r.at[a, k - 1])
            send(
                fpiece(src, across[a], a * fhalf, fhalf), fd_s.at[a, k - 1], fd_r.at[a, k - 1],
                (f, across[1 - a], t),
            )
    def corner_arrived(k):
        for a in range(2):
            piece = fpiece(fpeer(nf - k), corner, a * fhalf, fhalf)
            arrived(piece, fd_s.at[a, k - 1], fd_r.at[a, k - 1])

    @pl.loop(1, nf - 1)
    def _(k):
        corner_arrived(k)
        project(fpeer(nf - k))

    corner_arrived(nf - 1)
    at = block(fpeer(1))
    for i in range(TOKEN_TILES):
        span = pl.ds(i * tile, tile)
        product = jnp.dot(x[span, at], fac[t, at, :], preferred_element_type=F32)
        proj[t, :, span] = jnp.transpose(acc[span, :] + product).astype(BF16)
        send(proj.at[t, :, span], pj_s.at[i], pj_r.at[i], sibling)
    send(fac.at[t], fx_s, fx_r, sibling)
    relay("projection")
    for load in (*load_c, *load_s):
        load.wait()

    upper = rank // 2
    spans = (slice(0, upper), slice(upper, rank))

    def product(p, yy):
        at = pl.ds(pl.multiple_of(yy * side * width, side * width), side * width)
        both = jnp.dot(proj[p], c[p, :, at], preferred_element_type=F32)
        left, right = both[:, :width], both[:, width:]
        return jnp.where(rx == 0, left, right), jnp.where(rx == 0, right, left)

    def pass_part(s, m, a):
        send(part.at[s, m], rp_s.at[s, m], rp_r.at[s, m], (f, across[a], t), dst=recv.at[s, m])

    def got_part(s, m):
        arrived(recv.at[s, m], rp_s.at[s, m], rp_r.at[s, m])

    order = (t, 1 - t)
    for s, p in enumerate(order):
        if s == 1:
            for i in range(TOKEN_TILES):
                span = pl.ds(i * tile, tile)
                arrived(proj.at[1 - t, :, span], pj_s.at[i], pj_r.at[i])
        near_y, far = product(p, 1 - ry)
        for a in range(2):
            part[s, a] = far[spans[a]].astype(BF16)
            pass_part(s, a, a)
        part[s, 3] = near_y[spans[1]].astype(BF16)
        pass_part(s, 3, 1)
        keep[s, 0] = near_y[spans[0]]
        own[s], near_x = product(p, ry)
        part[s, 2] = near_x[spans[0]].astype(BF16)
        pass_part(s, 2, 0)
        keep[s, 1] = near_x[spans[1]]
    relay("products")

    def rank_rows(ff):
        return pl.ds(pl.multiple_of(ff * low_rows, low_rows), low_rows)

    for s in range(2):
        for a in range(2):
            got_part(s, a)
            part[s, 4 + a] = (keep[s, a] + recv[s, a].astype(F32)).astype(BF16)
            pass_part(s, 4 + a, 1 - a)
    relay("stage")
    for s in range(2):
        for a in range(2):
            got_part(s, 2 + a)
            got_part(s, 4 + a)
            total = own[s, spans[a], :] + recv[s, 2 + a].astype(F32) + recv[s, 4 + a].astype(F32)
            own[s, spans[a], :] = total
            mid[s, spans[a], :] = total.astype(BF16)
        for k in range(1, nf):
            onto = fpeer(k)
            piece = mid.at[s, rank_rows(onto), :]
            to_last = (onto == 0) | (onto == nf - 1)
            door = jnp.where(onto == 0, 1, nf - 2)
            send(
                piece, rf_s.at[s, k - 1], rf_r.at[s, k - 1], (onto, r, t), dst=recv_fs.at[s, k - 1],
                when=jnp.logical_not(to_last),
            )
            send(
                piece, re_s.at[s, k - 1], re_r.at[s, k - 1], (door, r, t), dst=recv_end.at[s, k - 1],
                when=to_last & (f != door),
            )
    relay("reduce")
    own_chunks(late=True, chunks=range(CHUNKS - 1))

    def dpiece(p, ff, rr, start=0, count=low_rows):
        at = pl.ds(pl.multiple_of(rr * width, width), width)
        ranks = pl.ds(pl.multiple_of(ff * low_rows + start, count), count)
        return dirs.at[p, ranks, at]

    for s, p in enumerate(order):
        for door, end, slots, slot in ((1, 0, range(nf - 2), nf - 2), (nf - 2, nf - 1, range(1, nf - 1), 0)):
            @pl.when(f == door)
            def _():
                ranks = slice(end * low_rows, (end + 1) * low_rows)
                total = own[s, ranks, :]
                for i in slots:
                    arrived(recv_end.at[s, i], re_s.at[s, i], re_r.at[s, i])
                    total = total + recv_end[s, i].astype(F32)
                joint[s] = total.astype(BF16)

            send(
                joint.at[s], rf_s.at[s, slot], rf_r.at[s, slot], (end, r, t), dst=recv_fs.at[s, slot],
                when=f == door,
            )
        for k in range(1, nf):
            @pl.when(inner | ((f == 0) & (k == nf - 1)) | ((f == nf - 1) & (k == 1)))
            def _():
                arrived(recv_fs.at[s, k - 1], rf_s.at[s, k - 1], rf_r.at[s, k - 1])
                own[s, rank_rows(f), :] = own[s, rank_rows(f), :] + recv_fs[s, k - 1].astype(F32)

        rounded = own[s, rank_rows(f), :].astype(BF16)
        low[p, :, lane] = rounded
        again = rounded.astype(F32)
        new_first = beta_first * moments[p, :, lane] + (1.0 - beta_first) * again
        new_second = beta_second * moments[2 + p, :, lane] + (1.0 - beta_second) * again * again
        direction = (new_first / jnp.sqrt(new_second)).astype(BF16)
        dirs[p, rank_rows(f), lane] = direction
        for k in range(1, nf):
            send(dpiece(p, f, r), dz_s.at[s, k - 1], dz_r.at[s, k - 1], (fpeer(k), r, t))
        for a in range(2):
            send(dpiece(p, f, r), dp_s.at[s, a, 0], dp_r.at[s, a, 0], (f, across[a], t))
        square = direction.astype(F32)
        square = square * square
        square = jnp.sum(square.reshape(low_rows // 8, 8, width), axis=0)
        sums[p] = square
    for k in range(1, nf):
        send(sums, sz_s.at[k - 1], sz_r.at[k - 1], (fpeer(k), r, t), dst=sums_z.at[k - 1])
    relay("directions")
    for s, p in enumerate(order):
        for k in range(1, nf):
            src = fpeer(nf - k)
            arrived(dpiece(p, src, r), dz_s.at[s, k - 1], dz_r.at[s, k - 1])
            for a in range(2):
                send(dpiece(p, src, r), dp_s.at[s, a, k], dp_r.at[s, a, k], (f, across[a], t))
    relay("gather_z")
    own_chunks(late=True, chunks=range(CHUNKS - 1, CHUNKS))
    for k in range(1, nf):
        arrived(sums_z.at[k - 1], sz_s.at[k - 1], sz_r.at[k - 1])
    total = sums[...]
    for k in range(1, nf):
        total = total + sums_z[k - 1]
    sums_r[0] = total
    for j in range(1, nr):
        send(sums_r.at[0], sr_s.at[j - 1], sr_r.at[j - 1], (f, rpeer(j), t), dst=sums_r.at[j])
    for s, p in enumerate(order):
        for k in range(nf):
            src = fpeer(nf - k) if k else f
            for a in range(2):
                arrived(dpiece(p, src, across[a]), dp_s.at[s, a, k], dp_r.at[s, a, k])
                send(
                    dpiece(p, src, across[a], a * low_half, low_half), dd_s.at[s, a, k], dd_r.at[s, a, k],
                    (f, across[1 - a], t),
                )
    for j in range(1, nr):
        send(low.at[:, :, lane], lw_s.at[j - 1], lw_r.at[j - 1], (f, rpeer(j), t))
    for j in range(1, nr):
        arrived(sums_r.at[j], sr_s.at[j - 1], sr_r.at[j - 1])
    total = sums_r[0]
    for j in range(1, nr):
        total = total + sums_r[j]
    sums_t[0] = total
    send(sums_t.at[0], st_s, st_r, sibling, dst=sums_t.at[1])
    arrived(fac.at[1 - t], fx_s, fx_r)
    relay("gather")

    for s, p in enumerate(order):
        for k in range(nf):
            src = fpeer(nf - k) if k else f
            for a in range(2):
                arrived(dpiece(p, src, corner, a * low_half, low_half), dd_s.at[s, a, k], dd_r.at[s, a, k])
    arrived(sums_t.at[1], st_s, st_r)
    total = sums_t[0] + sums_t[1]
    scales = [1.0 / jnp.sqrt(jnp.sum(total[p]) / entries + scale_floor) for p in range(2)]

    def update_of(p, at):
        return jnp.dot(fac[p, at, :], dirs[p], preferred_element_type=F32) * scales[p]

    def renew(p, start, count):
        at = pl.ds(pl.multiple_of(start, count), count)
        fresh[p, at, :] = (mast[p, at, :].astype(F32) - step_rate * update_of(p, at)).astype(BF16)

    unit = min(rows, 256)

    def renew_block(ff):
        for p in range(2):
            for i in range(rows // unit):
                renew(p, ff * rows + i * unit, unit)

    for p in range(2):
        for i in range(rows // unit):
            at = pl.ds(pl.multiple_of(f * rows + i * unit, unit), unit)
            update = update_of(p, at)
            span = pl.ds(i * unit, unit)
            fresh[p, at, :] = (mast[p, at, :].astype(F32) - step_rate * update).astype(BF16)
            upd[p, span, :] = update
    relay("end")
    def beside(j, ch, d):
        source, exists, _, _ = line[d]
        piece = mpiece(source(j), ch, other=True)
        arrived(piece, mp_s.at[d, j - 1, ch], mp_r.at[d, j - 1, ch])

    outer = [n for n in relays_last if n[0] in (1, nf - 1)]
    early = outer[:-CHUNKS + 1]

    def renew_outer(chunks, other):
        for j, ch in chunks:
            for d, (source, exists, _, _) in enumerate(line):
                @pl.when(exists(j) & last)
                def _():
                    if other:
                        beside(j, ch, d)
                    start, count = mrange(source(j), ch, other)
                    renew(ch % 2, start, count)

    renew_outer(early, False)
    @pl.loop(1, nf - 1)
    def _(j):
        for d, (source, exists, _, _) in enumerate(line):
            @pl.when(exists(j) & (inner | (j > 1)))
            def _():
                for ch in range(CHUNKS):
                    beside(j, ch, d)
                renew_block(source(j))

    for j in range(1, nr):
        rsrc = rpeer(nr - j)
        at = pl.ds(pl.multiple_of(rsrc * width, width), width)
        arrived(low.at[:, :, at], lw_s.at[j - 1], lw_r.at[j - 1])
    for p in range(2):
        again = low[p].astype(F32)
        moments[p] = beta_first * moments[p] + (1.0 - beta_first) * again
        moments[2 + p] = beta_second * moments[2 + p] + (1.0 - beta_second) * again * again

    renew_outer(early, True)
    renew_outer(outer[-CHUNKS + 1:], False)
    renew_outer(outer[-CHUNKS + 1:], True)
    for copy, when in started:
        guarded(copy.wait_send, when)


def gather_all(nf, nr, entries, normed_in, cotans, factors, firsts, seconds, masters):
    tokens, model = normed_in.shape
    cols = cotans[0].shape[1]
    rows, rank = factors[0].shape
    low_rows, width = rank // nf, cols // nr
    dma = pltpu.SemaphoreType.DMA
    anyspec = pl.BlockSpec(memory_space=pl.ANY)
    pair = lambda *shape: [dma(shape), dma(shape)]
    return pl.pallas_call(
        functools.partial(kernel, nf, nr, entries),
        out_shape=(
            pltpu.VMEM((2, model, cols), BF16),
            pltpu.VMEM((2, rows, cols), F32),
            pltpu.VMEM((4, low_rows, cols), F32),
        ),
        in_specs=[anyspec] * 11,
        out_specs=(pl.BlockSpec(memory_space=pltpu.VMEM),) * 3,
        scratch_shapes=[
            pltpu.VMEM((tokens, model), BF16),
            pltpu.VMEM((2, tokens, cols), BF16),
            pltpu.VMEM((2, model, rank), BF16),
            pltpu.VMEM((tokens, rank), F32),
            pltpu.VMEM((2, rank, tokens), BF16),
            pltpu.VMEM((2, 6, rank // 2, width), BF16),
            pltpu.VMEM((2, 6, rank // 2, width), BF16),
            pltpu.VMEM((2, 2, rank // 2, width), F32),
            pltpu.VMEM((2, rank, width), F32),
            pltpu.VMEM((2, rank, width), BF16),
            pltpu.VMEM((2, nf - 1, low_rows, width), BF16),
            pltpu.VMEM((2, nf - 1, low_rows, width), BF16),
            pltpu.VMEM((2, low_rows, width), BF16),
            pltpu.VMEM((2, low_rows, cols), BF16),
            pltpu.VMEM((2, rank, cols), BF16),
            pltpu.VMEM((2, model, cols), BF16),
            pltpu.VMEM((2, 8, width), F32),
            pltpu.VMEM((nf - 1, 2, 8, width), F32),
            pltpu.VMEM((nr, 2, 8, width), F32),
            pltpu.VMEM((2, 2, 8, width), F32),
            dma((10,)),
            *pair(nf - 1),
            *pair(2, nf - 1),
            *pair(2, nf - 1),
            dma,
            dma,
            *pair(TOKEN_TILES),
            *pair(2, 6),
            *pair(2, nf - 1),
            *pair(2, nf - 1),
            *pair(2, nf - 1),
            *pair(2, 2, nf),
            *pair(2, 2, nf),
            *pair(nr - 1),
            *pair(nf - 1),
            *pair(nr - 1),
            dma,
            dma,
            *pair(2, nf - 1, CHUNKS),
            *pair(2, nf - 1, CHUNKS),
        ],
        cost_estimate=pl.CostEstimate(
            flops=10 * tokens * model * rank, bytes_accessed=400 * 2**20, transcendentals=0
        ),
        compiler_params=pltpu.CompilerParams(
            collective_id=0, has_side_effects=True, vmem_limit_bytes=46 * 2**20
        ),
    )(normed_in, *cotans, *factors, *firsts, *seconds, *masters)


def finish_kernel(fresh, upd, moments, *rest):
    outs, sem = rest[:-1], rest[-1]
    pieces = [(upd.at[p], outs[p]) for p in range(2)]
    pieces += [(moments.at[i], outs[2 + i]) for i in range(4)]
    share = fresh.shape[1] // 4
    for p in range(2):
        for i in range(4):
            span = pl.ds(i * share, share)
            pieces.append((fresh.at[p, span, :], outs[6 + p].at[span, :]))
    copies = [pltpu.make_async_copy(src, dst, sem.at[i]) for i, (src, dst) in enumerate(pieces)]
    for copy in copies:
        copy.start()
    for copy in copies:
        copy.wait()


def finish(fresh, upd, moments):
    shape = jax.ShapeDtypeStruct
    anyspec = pl.BlockSpec(memory_space=pl.ANY)
    return pl.pallas_call(
        finish_kernel,
        out_shape=(
            *[shape(upd.shape[1:], F32)] * 2,
            *[shape(moments.shape[1:], F32)] * 4,
            *[shape(fresh.shape[1:], BF16)] * 2,
        ),
        in_specs=[pl.BlockSpec(memory_space=pltpu.VMEM)] * 3,
        out_specs=(anyspec,) * 8,
        scratch_shapes=[pltpu.SemaphoreType.DMA((14,))],
        cost_estimate=pl.CostEstimate(flops=0, bytes_accessed=14 * 2**20, transcendentals=0),
        compiler_params=pltpu.CompilerParams(vmem_limit_bytes=2**20),
    )(fresh, upd, moments)


def body(
    nf,
    nr,
    nt,
    normed_in,
    cotan_rec,
    cotan_gate,
    factor_rec,
    factor_gate,
    first_rec,
    first_gate,
    second_rec,
    second_gate,
    master_rec,
    master_gate,
):
    factors = (factor_rec, factor_gate)
    firsts = (first_rec, first_gate)
    seconds = (second_rec, second_gate)
    entries = float(factor_rec.shape[1] * cotan_rec.shape[1] * nt)
    return finish(
        *gather_all(
            nf, nr, entries, normed_in, (cotan_rec, cotan_gate), factors, firsts, seconds,
            (master_rec, master_gate),
        )
    )


def solution(mesh):
    nf, nr, nt = mesh.shape["fs"], mesh.shape["rep"], mesh.shape["tp"]
    rows = P("fs", "tp")
    return jax.shard_map(
        functools.partial(body, nf, nr, nt),
        mesh=mesh,
        in_specs=(
            P(("fs", "rep"), None),
            P(("fs", "rep"), "tp"),
            P(("fs", "rep"), "tp"),
            P("fs", None),
            P("fs", None),
            *[rows] * 6,
        ),
        out_specs=(*[rows] * 6, P(None, "tp"), P(None, "tp")),
        check_vma=False,
    )
```

```python
import functools

import jax
import jax.numpy as jnp
from jax import lax
from jax.experimental import pallas as pl
from jax.experimental.pallas import tpu as pltpu
from jax.sharding import PartitionSpec as P

beta_first = 0.8
beta_second = 0.9
scale_floor = 0.25
step_rate = 0.01

MESH = pl.DeviceIdType.MESH
F32 = jnp.float32
BF16 = jnp.bfloat16
TOKEN_TILES = 4
HALF_CHUNKS = 2
CHUNKS = 2 * HALF_CHUNKS
SHARES = {
    "projection": (0.0, 0.17, 0.08, 0.0),
    "products": (0.0, 0.25, 0.08, 0.0),
    "stage": (0.0, 0.33, 0.08, 0.0),
    "reduce": (0.5, 0.42, 0.17, 0.33),
    "directions": (0.58, 0.42, 0.25, 0.33),
    "gather_z": (0.58, 0.5, 0.33, 0.33),
    "gather": (0.83, 0.67, 0.67, 0.67),
    "end": (1.0, 1.0, 1.0, 1.0),
}


def kernel(
    nf,
    nr,
    entries,
    x_hbm,
    c0_hbm,
    c1_hbm,
    fac0_hbm,
    fac1_hbm,
    first0,
    first1,
    second0,
    second1,
    mast0_hbm,
    mast1_hbm,
    fresh,
    upd,
    moments,
    x,
    c,
    fac,
    acc,
    proj,
    part,
    recv,
    keep,
    own,
    mid,
    recv_fs,
    recv_end,
    joint,
    low,
    dirs,
    mast,
    sums,
    sums_z,
    sums_r,
    sums_t,
    local_sem,
    fz_s,
    fz_r,
    fp_s,
    fp_r,
    fd_s,
    fd_r,
    fx_s,
    fx_r,
    pj_s,
    pj_r,
    rp_s,
    rp_r,
    rf_s,
    rf_r,
    re_s,
    re_r,
    dz_s,
    dz_r,
    dp_s,
    dp_r,
    dd_s,
    dd_r,
    lw_s,
    lw_r,
    sz_s,
    sz_r,
    sr_s,
    sr_r,
    st_s,
    st_r,
    mz_s,
    mz_r,
    mp_s,
    mp_r,
):
    f, r, t = lax.axis_index("fs"), lax.axis_index("rep"), lax.axis_index("tp")
    tokens = x.shape[0]
    rank, cols = dirs.shape[1], dirs.shape[2]
    rows = fac0_hbm.shape[0]
    half, quarter = rows // 2, rows // nr
    low_rows = rank // nf
    low_half = low_rows // 2
    width = cols // nr
    tile = tokens // TOKEN_TILES
    side = nr // 2
    rx, ry = lax.rem(r, side), r // side
    across = (ry * side + 1 - rx, (1 - ry) * side + rx)
    corner = (1 - ry) * side + 1 - rx
    sibling = (f, r, 1 - t)

    def fpeer(k):
        return lax.rem(f + k, nf)

    def rpeer(k):
        return lax.rem(r + k, nr)

    def block(ff):
        return pl.ds(pl.multiple_of(ff * rows, rows), rows)

    mine = fac.at[t, block(f), :]

    @pl.when(t == 0)
    def _():
        pltpu.make_async_copy(fac0_hbm, mine, local_sem.at[0]).start()

    @pl.when(t != 0)
    def _():
        pltpu.make_async_copy(fac1_hbm, mine, local_sem.at[0]).start()

    load_m = [
        pltpu.make_async_copy(mast0_hbm, upd.at[0], local_sem.at[8]),
        pltpu.make_async_copy(mast1_hbm, upd.at[1], local_sem.at[9]),
    ]
    load_x = pltpu.make_async_copy(x_hbm, x, local_sem.at[1])
    for load in (*load_m, load_x):
        load.start()
    load_c = [
        pltpu.make_async_copy(c0_hbm, c.at[0], local_sem.at[2]),
        pltpu.make_async_copy(c1_hbm, c.at[1], local_sem.at[3]),
    ]
    lane = pl.ds(pl.multiple_of(r * width, width), width)
    load_s = [
        pltpu.make_async_copy(src, moments.at[i], local_sem.at[4 + i])
        for i, src in enumerate((first0, first1, second0, second1))
    ]
    for load in (*load_c, *load_s):
        load.start()

    barrier = pltpu.get_barrier_semaphore()
    for k in range(1, nf):
        pl.semaphore_signal(barrier, inc=1, device_id=(fpeer(k), r, t), device_id_type=MESH)
    for k in range(1, nr):
        pl.semaphore_signal(barrier, inc=1, device_id=(f, rpeer(k), t), device_id_type=MESH)
    pl.semaphore_signal(barrier, inc=1, device_id=sibling, device_id_type=MESH)
    pl.semaphore_wait(barrier, nf + nr - 1)

    started = []

    def remote(src, dst, s_sem, r_sem, device):
        return pltpu.make_async_remote_copy(
            src_ref=src, dst_ref=dst, send_sem=s_sem, recv_sem=r_sem,
            device_id=device, device_id_type=MESH,
        )

    def guarded(action, when):
        if when is None:
            action()
        else:
            pl.when(when)(lambda: action())

    def send(ref, s_sem, r_sem, device, dst=None, when=None):
        copy = remote(ref, ref if dst is None else dst, s_sem, r_sem, device)
        guarded(copy.start, when)
        started.append((copy, when))

    def arrived(ref, s_sem, r_sem, when=None):
        guarded(remote(ref, ref, s_sem, r_sem, sibling).wait_recv, when)

    def fpiece(ff, rr, start=0, count=quarter):
        at = pl.multiple_of(ff * rows + rr * quarter + start, count)
        return fac.at[t, pl.ds(at, count), :]

    pltpu.make_async_copy(fac0_hbm, mine, local_sem.at[0]).wait()
    for k in range(1, nf):
        send(fpiece(f, r), fz_s.at[k - 1], fz_r.at[k - 1], (fpeer(k), r, t))

    chunk = half // HALF_CHUNKS
    line = (
        (lambda j: lax.rem(f + nf - j, nf), lambda j: f >= j, fpeer(1), f < nf - 1),
        (lambda j: lax.rem(f + j, nf), lambda j: f < nf - j, fpeer(nf - 1), f > 0),
    )

    def mrange(ff, ch, other=False):
        h = rx if ch % 2 == 0 else ry
        if other:
            h = 1 - h
        return ff * rows + h * half + (ch // 2) * chunk, chunk

    def mpiece(ff, ch, other=False):
        start, count = mrange(ff, ch, other)
        return mast.at[ch % 2, pl.ds(pl.multiple_of(start, count), count), :]

    def own_chunks(late, chunks=range(CHUNKS)):
        for ch in chunks:
            for d, (_, _, onto, there) in enumerate(line):
                to_end = f == (nf - 2 if d == 0 else 1)
                when = there
                if late:
                    when = there & to_end
                elif ch >= CHUNKS // 2:
                    when = there & jnp.logical_not(to_end)
                if ch >= CHUNKS // 2 or not late:
                    send(mpiece(f, ch), mz_s.at[d, 0, ch], mz_r.at[d, 0, ch], (onto, r, t), when=when)

    for p in range(2):
        load_m[p].wait()
        mast[p, block(f), :] = upd[p].astype(BF16)
    own_chunks(late=False)

    relays = [(j, ch) for j in range(1, nf) for ch in range(CHUNKS)]
    late = [(1, ch) for ch in range(CHUNKS // 2, CHUNKS)]
    final = relays[-(CHUNKS // 2):]
    relays_last = [n for n in relays if n not in late and n not in final]
    relays_last.insert(len(relays_last) - CHUNKS // 2, late[0])
    relays_last += late[1:] + final
    done = [0, 0, 0, 0]
    last = jnp.logical_or(f == 0, f == nf - 1)
    inner = jnp.logical_not(last)

    def land(j, ch, when):
        for d, (source, exists, _, _) in enumerate(line):
            piece = mpiece(source(j), ch)
            arrived(piece, mz_s.at[d, j - 1, ch], mz_r.at[d, j - 1, ch], when=exists(j) & when)

    def onward(j, ch, ending):
        if j == nf - 1:
            return
        for d, (source, exists, onto, there) in enumerate(line):
            to_end = f == (nf - 2 if d == 0 else 1)
            if not ending:
                to_end = jnp.logical_not(to_end)
            send(
                mpiece(source(j), ch), mz_s.at[d, j, ch], mz_r.at[d, j, ch], (onto, r, t),
                when=exists(j) & there & inner & to_end,
            )

    def aside(j, ch, when):
        for d, (source, exists, _, _) in enumerate(line):
            piece = mpiece(source(j), ch)
            send(
                piece, mp_s.at[d, j - 1, ch], mp_r.at[d, j - 1, ch], (f, across[ch % 2], t),
                when=exists(j) & when,
            )

    def relay(point):
        ends = [max(d, round(share * len(relays))) for d, share in zip(done, SHARES[point])]
        for n in range(done[0], ends[0]):
            land(*relays_last[n], last)
            aside(*relays_last[n], last)
        landed = max(done[1:])
        for n in range(min(done[1:]), max(ends[1:])):
            if n >= landed:
                land(*relays[n], inner)
            if done[1] <= n < ends[1]:
                onward(*relays[n], True)
            if done[2] <= n < ends[2]:
                onward(*relays[n], False)
            if done[3] <= n < ends[3]:
                aside(*relays[n], inner)
        done[:] = ends

    def project(ff, first=False):
        at = block(ff)
        for i in range(TOKEN_TILES):
            span = pl.ds(i * tile, tile)
            product = jnp.dot(x[span, at], fac[t, at, :], preferred_element_type=F32)
            acc[span, :] = product if first else acc[span, :] + product

    load_x.wait()
    project(f, first=True)

    for k in range(1, nf):
        src = fpeer(nf - k)
        arrived(fpiece(src, r), fz_s.at[k - 1], fz_r.at[k - 1])
        for a in range(2):
            send(fpiece(src, r), fp_s.at[a, k - 1], fp_r.at[a, k - 1], (f, across[a], t))
    fhalf = quarter // 2
    for k in range(1, nf):
        src = fpeer(nf - k)
        for a in range(2):
            arrived(fpiece(src, across[a]), fp_s.at[a, k - 1], fp_r.at[a, k - 1])
            send(
                fpiece(src, across[a], a * fhalf, fhalf), fd_s.at[a, k - 1], fd_r.at[a, k - 1],
                (f, across[1 - a], t),
            )
    def corner_arrived(k):
        for a in range(2):
            piece = fpiece(fpeer(nf - k), corner, a * fhalf, fhalf)
            arrived(piece, fd_s.at[a, k - 1], fd_r.at[a, k - 1])

    @pl.loop(1, nf - 1)
    def _(k):
        corner_arrived(k)
        project(fpeer(nf - k))

    corner_arrived(nf - 1)
    at = block(fpeer(1))
    for i in range(TOKEN_TILES):
        span = pl.ds(i * tile, tile)
        product = jnp.dot(x[span, at], fac[t, at, :], preferred_element_type=F32)
        proj[t, :, span] = jnp.transpose(acc[span, :] + product).astype(BF16)
        send(proj.at[t, :, span], pj_s.at[i], pj_r.at[i], sibling)
    send(fac.at[t], fx_s, fx_r, sibling)
    relay("projection")
    for load in (*load_c, *load_s):
        load.wait()

    upper = rank // 2
    spans = (slice(0, upper), slice(upper, rank))

    def product(p, yy):
        at = pl.ds(pl.multiple_of(yy * side * width, side * width), side * width)
        both = jnp.dot(proj[p], c[p, :, at], preferred_element_type=F32)
        left, right = both[:, :width], both[:, width:]
        return jnp.where(rx == 0, left, right), jnp.where(rx == 0, right, left)

    def pass_part(s, m, a):
        send(part.at[s, m], rp_s.at[s, m], rp_r.at[s, m], (f, across[a], t), dst=recv.at[s, m])

    def got_part(s, m):
        arrived(recv.at[s, m], rp_s.at[s, m], rp_r.at[s, m])

    order = (t, 1 - t)
    for s, p in enumerate(order):
        if s == 1:
            for i in range(TOKEN_TILES):
                span = pl.ds(i * tile, tile)
                arrived(proj.at[1 - t, :, span], pj_s.at[i], pj_r.at[i])
        near_y, far = product(p, 1 - ry)
        for a in range(2):
            part[s, a] = far[spans[a]].astype(BF16)
            pass_part(s, a, a)
        part[s, 3] = near_y[spans[1]].astype(BF16)
        pass_part(s, 3, 1)
        keep[s, 0] = near_y[spans[0]]
        own[s], near_x = product(p, ry)
        part[s, 2] = near_x[spans[0]].astype(BF16)
        pass_part(s, 2, 0)
        keep[s, 1] = near_x[spans[1]]
    relay("products")

    def rank_rows(ff):
        return pl.ds(pl.multiple_of(ff * low_rows, low_rows), low_rows)

    for s in range(2):
        for a in range(2):
            got_part(s, a)
            part[s, 4 + a] = (keep[s, a] + recv[s, a].astype(F32)).astype(BF16)
            pass_part(s, 4 + a, 1 - a)
    relay("stage")
    for s in range(2):
        for a in range(2):
            got_part(s, 2 + a)
            got_part(s, 4 + a)
            total = own[s, spans[a], :] + recv[s, 2 + a].astype(F32) + recv[s, 4 + a].astype(F32)
            own[s, spans[a], :] = total
            mid[s, spans[a], :] = total.astype(BF16)
        for k in range(1, nf):
            onto = fpeer(k)
            piece = mid.at[s, rank_rows(onto), :]
            to_last = (onto == 0) | (onto == nf - 1)
            door = jnp.where(onto == 0, 1, nf - 2)
            send(
                piece, rf_s.at[s, k - 1], rf_r.at[s, k - 1], (onto, r, t), dst=recv_fs.at[s, k - 1],
                when=jnp.logical_not(to_last),
            )
            send(
                piece, re_s.at[s, k - 1], re_r.at[s, k - 1], (door, r, t), dst=recv_end.at[s, k - 1],
                when=to_last & (f != door),
            )
    relay("reduce")
    own_chunks(late=True, chunks=range(CHUNKS - 1))

    def dpiece(p, ff, rr, start=0, count=low_rows):
        at = pl.ds(pl.multiple_of(rr * width, width), width)
        ranks = pl.ds(pl.multiple_of(ff * low_rows + start, count), count)
        return dirs.at[p, ranks, at]

    for s, p in enumerate(order):
        for door, end, slots, slot in ((1, 0, range(nf - 2), nf - 2), (nf - 2, nf - 1, range(1, nf - 1), 0)):
            @pl.when(f == door)
            def _():
                ranks = slice(end * low_rows, (end + 1) * low_rows)
                total = own[s, ranks, :]
                for i in slots:
                    arrived(recv_end.at[s, i], re_s.at[s, i], re_r.at[s, i])
                    total = total + recv_end[s, i].astype(F32)
                joint[s] = total.astype(BF16)

            send(
                joint.at[s], rf_s.at[s, slot], rf_r.at[s, slot], (end, r, t), dst=recv_fs.at[s, slot],
                when=f == door,
            )
        for k in range(1, nf):
            @pl.when(inner | ((f == 0) & (k == nf - 1)) | ((f == nf - 1) & (k == 1)))
            def _():
                arrived(recv_fs.at[s, k - 1], rf_s.at[s, k - 1], rf_r.at[s, k - 1])
                own[s, rank_rows(f), :] = own[s, rank_rows(f), :] + recv_fs[s, k - 1].astype(F32)

        rounded = own[s, rank_rows(f), :].astype(BF16)
        low[p, :, lane] = rounded
        again = rounded.astype(F32)
        new_first = beta_first * moments[p, :, lane] + (1.0 - beta_first) * again
        new_second = beta_second * moments[2 + p, :, lane] + (1.0 - beta_second) * again * again
        direction = (new_first / jnp.sqrt(new_second)).astype(BF16)
        dirs[p, rank_rows(f), lane] = direction
        for k in range(1, nf):
            send(dpiece(p, f, r), dz_s.at[s, k - 1], dz_r.at[s, k - 1], (fpeer(k), r, t))
        for a in range(2):
            send(dpiece(p, f, r), dp_s.at[s, a, 0], dp_r.at[s, a, 0], (f, across[a], t))
        square = direction.astype(F32)
        square = square * square
        square = jnp.sum(square.reshape(low_rows // 8, 8, width), axis=0)
        sums[p] = square
    for k in range(1, nf):
        send(sums, sz_s.at[k - 1], sz_r.at[k - 1], (fpeer(k), r, t), dst=sums_z.at[k - 1])
    relay("directions")
    for s, p in enumerate(order):
        for k in range(1, nf):
            src = fpeer(nf - k)
            arrived(dpiece(p, src, r), dz_s.at[s, k - 1], dz_r.at[s, k - 1])
            for a in range(2):
                send(dpiece(p, src, r), dp_s.at[s, a, k], dp_r.at[s, a, k], (f, across[a], t))
    relay("gather_z")
    own_chunks(late=True, chunks=range(CHUNKS - 1, CHUNKS))
    for k in range(1, nf):
        arrived(sums_z.at[k - 1], sz_s.at[k - 1], sz_r.at[k - 1])
    total = sums[...]
    for k in range(1, nf):
        total = total + sums_z[k - 1]
    sums_r[0] = total
    for j in range(1, nr):
        send(sums_r.at[0], sr_s.at[j - 1], sr_r.at[j - 1], (f, rpeer(j), t), dst=sums_r.at[j])
    for s, p in enumerate(order):
        for k in range(nf):
            src = fpeer(nf - k) if k else f
            for a in range(2):
                arrived(dpiece(p, src, across[a]), dp_s.at[s, a, k], dp_r.at[s, a, k])
                send(
                    dpiece(p, src, across[a], a * low_half, low_half), dd_s.at[s, a, k], dd_r.at[s, a, k],
                    (f, across[1 - a], t),
                )
    for j in range(1, nr):
        send(low.at[:, :, lane], lw_s.at[j - 1], lw_r.at[j - 1], (f, rpeer(j), t))
    for j in range(1, nr):
        arrived(sums_r.at[j], sr_s.at[j - 1], sr_r.at[j - 1])
    total = sums_r[0]
    for j in range(1, nr):
        total = total + sums_r[j]
    sums_t[0] = total
    send(sums_t.at[0], st_s, st_r, sibling, dst=sums_t.at[1])
    arrived(fac.at[1 - t], fx_s, fx_r)
    relay("gather")

    for s, p in enumerate(order):
        for k in range(nf):
            src = fpeer(nf - k) if k else f
            for a in range(2):
                arrived(dpiece(p, src, corner, a * low_half, low_half), dd_s.at[s, a, k], dd_r.at[s, a, k])
    arrived(sums_t.at[1], st_s, st_r)
    total = sums_t[0] + sums_t[1]
    scales = [1.0 / jnp.sqrt(jnp.sum(total[p]) / entries + scale_floor) for p in range(2)]

    def update_of(p, at):
        return jnp.dot(fac[p, at, :], dirs[p], preferred_element_type=F32) * scales[p]

    def renew(p, start, count):
        at = pl.ds(pl.multiple_of(start, count), count)
        fresh[p, at, :] = (mast[p, at, :].astype(F32) - step_rate * update_of(p, at)).astype(BF16)

    unit = min(rows, 256)

    def renew_block(ff):
        for p in range(2):
            for i in range(rows // unit):
                renew(p, ff * rows + i * unit, unit)

    for p in range(2):
        for i in range(rows // unit):
            at = pl.ds(pl.multiple_of(f * rows + i * unit, unit), unit)
            update = update_of(p, at)
            span = pl.ds(i * unit, unit)
            fresh[p, at, :] = (mast[p, at, :].astype(F32) - step_rate * update).astype(BF16)
            upd[p, span, :] = update
    relay("end")
    def beside(j, ch, d):
        source, exists, _, _ = line[d]
        piece = mpiece(source(j), ch, other=True)
        arrived(piece, mp_s.at[d, j - 1, ch], mp_r.at[d, j - 1, ch])

    outer = [n for n in relays_last if n[0] in (1, nf - 1)]
    early = outer[:-CHUNKS + 1]

    def renew_outer(chunks, other):
        for j, ch in chunks:
            for d, (source, exists, _, _) in enumerate(line):
                @pl.when(exists(j) & last)
                def _():
                    if other:
                        beside(j, ch, d)
                    start, count = mrange(source(j), ch, other)
                    renew(ch % 2, start, count)

    renew_outer(early, False)
    @pl.loop(1, nf - 1)
    def _(j):
        for d, (source, exists, _, _) in enumerate(line):
            @pl.when(exists(j) & (inner | (j > 1)))
            def _():
                for ch in range(CHUNKS):
                    beside(j, ch, d)
                renew_block(source(j))

    for j in range(1, nr):
        rsrc = rpeer(nr - j)
        at = pl.ds(pl.multiple_of(rsrc * width, width), width)
        arrived(low.at[:, :, at], lw_s.at[j - 1], lw_r.at[j - 1])
    for p in range(2):
        again = low[p].astype(F32)
        moments[p] = beta_first * moments[p] + (1.0 - beta_first) * again
        moments[2 + p] = beta_second * moments[2 + p] + (1.0 - beta_second) * again * again

    renew_outer(early, True)
    renew_outer(outer[-CHUNKS + 1:], False)
    renew_outer(outer[-CHUNKS + 1:], True)
    for copy, when in started:
        guarded(copy.wait_send, when)


def gather_all(nf, nr, entries, normed_in, cotans, factors, firsts, seconds, masters):
    tokens, model = normed_in.shape
    cols = cotans[0].shape[1]
    rows, rank = factors[0].shape
    low_rows, width = rank // nf, cols // nr
    dma = pltpu.SemaphoreType.DMA
    anyspec = pl.BlockSpec(memory_space=pl.ANY)
    pair = lambda *shape: [dma(shape), dma(shape)]
    return pl.pallas_call(
        functools.partial(kernel, nf, nr, entries),
        out_shape=(
            pltpu.VMEM((2, model, cols), BF16),
            pltpu.VMEM((2, rows, cols), F32),
            pltpu.VMEM((4, low_rows, cols), F32),
        ),
        in_specs=[anyspec] * 11,
        out_specs=(pl.BlockSpec(memory_space=pltpu.VMEM),) * 3,
        scratch_shapes=[
            pltpu.VMEM((tokens, model), BF16),
            pltpu.VMEM((2, tokens, cols), BF16),
            pltpu.VMEM((2, model, rank), BF16),
            pltpu.VMEM((tokens, rank), F32),
            pltpu.VMEM((2, rank, tokens), BF16),
            pltpu.VMEM((2, 6, rank // 2, width), BF16),
            pltpu.VMEM((2, 6, rank // 2, width), BF16),
            pltpu.VMEM((2, 2, rank // 2, width), F32),
            pltpu.VMEM((2, rank, width), F32),
            pltpu.VMEM((2, rank, width), BF16),
            pltpu.VMEM((2, nf - 1, low_rows, width), BF16),
            pltpu.VMEM((2, nf - 1, low_rows, width), BF16),
            pltpu.VMEM((2, low_rows, width), BF16),
            pltpu.VMEM((2, low_rows, cols), BF16),
            pltpu.VMEM((2, rank, cols), BF16),
            pltpu.VMEM((2, model, cols), BF16),
            pltpu.VMEM((2, 8, width), F32),
            pltpu.VMEM((nf - 1, 2, 8, width), F32),
            pltpu.VMEM((nr, 2, 8, width), F32),
            pltpu.VMEM((2, 2, 8, width), F32),
            dma((10,)),
            *pair(nf - 1),
            *pair(2, nf - 1),
            *pair(2, nf - 1),
            dma,
            dma,
            *pair(TOKEN_TILES),
            *pair(2, 6),
            *pair(2, nf - 1),
            *pair(2, nf - 1),
            *pair(2, nf - 1),
            *pair(2, 2, nf),
            *pair(2, 2, nf),
            *pair(nr - 1),
            *pair(nf - 1),
            *pair(nr - 1),
            dma,
            dma,
            *pair(2, nf - 1, CHUNKS),
            *pair(2, nf - 1, CHUNKS),
        ],
        cost_estimate=pl.CostEstimate(
            flops=10 * tokens * model * rank, bytes_accessed=400 * 2**20, transcendentals=0
        ),
        compiler_params=pltpu.CompilerParams(
            collective_id=0, has_side_effects=True, vmem_limit_bytes=46 * 2**20
        ),
    )(normed_in, *cotans, *factors, *firsts, *seconds, *masters)


def finish_kernel(fresh, upd, moments, *rest):
    outs, sem = rest[:-1], rest[-1]
    pieces = [(upd.at[p], outs[p]) for p in range(2)]
    pieces += [(moments.at[i], outs[2 + i]) for i in range(4)]
    share = fresh.shape[1] // 4
    for p in range(2):
        for i in range(4):
            span = pl.ds(i * share, share)
            pieces.append((fresh.at[p, span, :], outs[6 + p].at[span, :]))
    copies = [pltpu.make_async_copy(src, dst, sem.at[i]) for i, (src, dst) in enumerate(pieces)]
    for copy in copies:
        copy.start()
    for copy in copies:
        copy.wait()


def finish(fresh, upd, moments):
    shape = jax.ShapeDtypeStruct
    anyspec = pl.BlockSpec(memory_space=pl.ANY)
    return pl.pallas_call(
        finish_kernel,
        out_shape=(
            *[shape(upd.shape[1:], F32)] * 2,
            *[shape(moments.shape[1:], F32)] * 4,
            *[shape(fresh.shape[1:], BF16)] * 2,
        ),
        in_specs=[pl.BlockSpec(memory_space=pltpu.VMEM)] * 3,
        out_specs=(anyspec,) * 8,
        scratch_shapes=[pltpu.SemaphoreType.DMA((14,))],
        cost_estimate=pl.CostEstimate(flops=0, bytes_accessed=14 * 2**20, transcendentals=0),
        compiler_params=pltpu.CompilerParams(vmem_limit_bytes=2**20),
    )(fresh, upd, moments)


def body(
    nf,
    nr,
    nt,
    normed_in,
    cotan_rec,
    cotan_gate,
    factor_rec,
    factor_gate,
    first_rec,
    first_gate,
    second_rec,
    second_gate,
    master_rec,
    master_gate,
):
    factors = (factor_rec, factor_gate)
    firsts = (first_rec, first_gate)
    seconds = (second_rec, second_gate)
    entries = float(factor_rec.shape[1] * cotan_rec.shape[1] * nt)
    return finish(
        *gather_all(
            nf, nr, entries, normed_in, (cotan_rec, cotan_gate), factors, firsts, seconds,
            (master_rec, master_gate),
        )
    )


def solution(mesh):
    nf, nr, nt = mesh.shape["fs"], mesh.shape["rep"], mesh.shape["tp"]
    rows = P("fs", "tp")
    return jax.shard_map(
        functools.partial(body, nf, nr, nt),
        mesh=mesh,
        in_specs=(
            P(("fs", "rep"), None),
            P(("fs", "rep"), "tp"),
            P(("fs", "rep"), "tp"),
            P("fs", None),
            P("fs", None),
            *[rows] * 6,
        ),
        out_specs=(*[rows] * 6, P(None, "tp"), P(None, "tp")),
        check_vma=False,
    )
```
